256 devices in a mesh: ep: 64 (over z, x, core), tp: 4 (over y).
Axes of the slice: x: 4, y: 4, z: 8, core: 2. Of those that a mesh axis runs over, the one named last changes fastest.
Arguments:
- filter_value: bfloat16 [65536, 1024], P(('ep', 'tp')), may hold values from -6 to 6
- filter_gate: bfloat16 [65536, 1024], P(('ep', 'tp')), may hold values from -9 to 9
- filter_taps: float32 [31, 1024], replicated, may hold values from -1 to 1
- filter_bias: float32 [1024], replicated, may hold values from -3 to 3
- norm_gain: float32 [1024], replicated, may hold values from 0.1 to 1.9
- norm_shift: float32 [1024], replicated, may hold values from -3 to 3
- out_weight: bfloat16 [1024, 2048], replicated, may hold values from -0.1875 to 0.1875
- out_bias: float32 [2048], replicated, may hold values from -3 to 3
- expert_input: bfloat16 [16384, 2048], P('ep'), may hold values from -6 to 6
- expert_gain: float32 [2048], replicated, may hold values from 0.1 to 1.9
- route_experts: int32 [16384, 2], P('ep'), may hold values from 0 to 63, all different within a row; in each aligned block of 256 rows (0 to 255, 256 to 511, ...) at most 16 rows name the same one
- route_weights: float32 [16384, 2], P('ep'), may hold values from 0.2 to 1
- gate_weights: bfloat16 [64, 2048, 2048], P('ep', None, 'tp'), may hold values from -0.375 to 0.375
- up_weights: bfloat16 [64, 2048, 2048], P('ep', None, 'tp'), may hold values from -0.375 to 0.375
- down_weights: bfloat16 [64, 2048, 2048], P('ep', 'tp'), may hold values from -0.0234375 to 0.0234375
Outputs:
- mixer_out: bfloat16 [65536, 2048], P(('ep', 'tp'))
- expert_out: bfloat16 [16384, 2048], P('ep', 'tp')
The draws below stay inside these ranges and needn't reach their ends.
Inputs may be any that keep to these rules, and one draw needn't show every extreme that they name: `route_experts`: each row names 2 different experts. Within the rows of one index of ep (aligned blocks of 256 rows) no expert is named by more than 16 rows, a bound that some block reaches.
All inputs are finite; a program needn't handle non-finite values.
Results may differ from the reference program's by a relative error of at most 0.012.
Values may be sent and summed in bfloat16 or wider, within the bound.
A program may use at most 128 MiB of HBM per device.

```python
import math
import jax
import jax.numpy as jnp
import numpy as np
from jax import lax

D = 2048
CHANNELS = 1024
TAPS = 31
HIDDEN_SIZE = 2048
TOPK = 2
ROUTE_DEV = 256
EXPERTS = 64
CAPACITY = 16
MIX_TOKENS = 65536
ROUTE_TOKENS = 16384
N_EP = 64
N_TP = 4


def level_of(rng, shape, split, low, top_value):
    def one(axis_at, parts):
        draws = jax.random.uniform(jax.random.fold_in(jax.random.fold_in(rng, 6), axis_at), (parts,), jnp.float32, low / len(split), top_value / len(split))
        return jnp.repeat(jnp.exp(draws), shape[axis_at] // parts).reshape((-1,) + (1,) * (len(shape) - axis_at - 1))

    factor_of = one(*split[0])
    for cut in split[1:]:
        factor_of = factor_of * one(*cut)
    return factor_of


def deal_out(stream_key, own, number, rows, count, top, reach, lean):
    sequence = jax.random.permutation(stream_key, count)
    heavy_load, ordinary = shares(count, rows * top, reach, lean, True), shares(count, rows * top, reach, lean, False)
    places = jnp.arange(count)

    def named(tallies, turn):
        used = int((tallies > 0).sum())
        fixed = max(1, used // 4)
        passed = fixed + (places - fixed + turn * (used - fixed)) % max(1, count - fixed)
        return jnp.zeros((count,), jnp.int32).at[sequence[jnp.where(places < fixed, places, passed)]].set(jnp.asarray(tallies, jnp.int32))

    tallies = jnp.where(number % 4 == 0, named(heavy_load, number // 4), named(ordinary, number - number // 4 - 1))
    mixed = jax.random.permutation(jax.random.fold_in(own, 3), count)
    giver, taker = mixed[0:count // 2 * 2:2], mixed[1:count // 2 * 2:2]
    margin = jnp.minimum(tallies[giver] - 1, reach - tallies[taker]) // 2
    margin = jnp.where((giver == sequence[0]) | (taker == sequence[0]) | (tallies[taker] == 0), 0, jnp.maximum(margin, 0))
    passed = jax.random.randint(jax.random.fold_in(own, 4), (count // 2,), 0, 1 << 20) % (margin + 1)
    tallies = tallies.at[giver].add(-passed).at[taker].add(passed)
    items = jnp.searchsorted(jnp.cumsum(tallies), jnp.arange(rows * top), side="right").astype(jnp.int32)
    grid = items.reshape(top, rows).T
    grid = grid[jax.random.permutation(jax.random.fold_in(own, 1), rows)]
    turn = jax.random.randint(jax.random.fold_in(own, 2), (rows, 1), 0, top)
    return jnp.take_along_axis(grid, (jnp.arange(top)[None, :] + turn) % top, axis=1)


def shares(number_of, total, bound, slope, full):
    loads = [(1 << 20) // math.isqrt(grade ** slope) + 1 for grade in range(1, number_of + 1)]
    largest = bound if full else min(bound, max(-(-total // number_of), total * loads[0] // sum(loads)))
    least = 1 if total - largest >= number_of - 1 else 0
    given, spare = [largest] + [least] * (number_of - 1), total - largest - least * (number_of - 1)
    while spare > 0:
        movable = [i for i in range(1, number_of) if given[i] < largest] or [i for i in range(1, number_of) if given[i] < bound]
        whole, budget = sum([loads[i] for i in movable]), spare
        for i in movable:
            extra = min(bound - given[i], max(1, budget * loads[i] // whole), spare)
            given[i] = given[i] + extra
            spare = spare - extra
    return np.array(given)


def bell_draw(key, extent, width, reach, split=(), held_as=jnp.bfloat16):
    values = width * jax.random.normal(key, extent, jnp.float32)
    if split:
        values = values * level_of(key, extent, split, -0.22, 0.18)
    return jnp.clip(values, -reach, reach).astype(held_as)


def setup_inputs(seed: int = 0) -> dict:
    key_of = jax.random.split(jax.random.key(seed), 16)
    filter_value = bell_draw(key_of[0], (MIX_TOKENS, CHANNELS), 1.0, 6.0, ((0, 256),))
    filter_gate = bell_draw(key_of[1], (MIX_TOKENS, CHANNELS), 1.5, 9.0, ((0, 256),))
    filter_taps = bell_draw(key_of[2], (TAPS, CHANNELS), TAPS ** -0.5, 1.0, (), jnp.float32)
    filter_bias = bell_draw(key_of[3], (CHANNELS,), 0.5, 3.0, (), jnp.float32)
    norm_gain = jnp.clip(1.0 + 0.18 * jax.random.normal(key_of[4], (CHANNELS,), jnp.float32), 0.1, 1.9)
    norm_shift = bell_draw(key_of[5], (CHANNELS,), 0.5, 3.0, (), jnp.float32)
    out_weight = bell_draw(key_of[6], (CHANNELS, D), CHANNELS ** -0.5, 0.1875)
    out_bias = bell_draw(key_of[7], (D,), 0.5, 3.0, (), jnp.float32)
    expert_input = bell_draw(key_of[8], (ROUTE_TOKENS, D), 1.0, 6.0, ((0, 64),))
    expert_gain = jnp.clip(1.0 + 0.18 * jax.random.normal(key_of[9], (D,), jnp.float32), 0.1, 1.9)
    route_experts_keys = jax.random.split(jax.random.fold_in(key_of[10], 1), ROUTE_TOKENS // ROUTE_DEV)
    route_experts_turns = jax.random.permutation(jax.random.fold_in(key_of[10], 3), ROUTE_TOKENS // ROUTE_DEV)
    route_experts = jax.vmap(lambda own, number: deal_out(jax.random.fold_in(key_of[10], 2), own, number, ROUTE_DEV, EXPERTS, TOPK, CAPACITY, 2))(route_experts_keys, route_experts_turns).reshape((ROUTE_TOKENS, TOPK))
    route_weights = jnp.clip(0.2 + 0.8 * jax.random.uniform(key_of[11], (ROUTE_TOKENS, TOPK), jnp.float32) ** level_of(key_of[11], (ROUTE_TOKENS, TOPK), ((0, 64),), -0.2, 0.2), 0.2, 1.0)
    gate_weights = bell_draw(key_of[12], (EXPERTS, D, HIDDEN_SIZE), (D // 8) ** -0.5, 0.375, ((0, 64), (2, 4)))
    up_weights = bell_draw(key_of[13], (EXPERTS, D, HIDDEN_SIZE), (D // 8) ** -0.5, 0.375, ((0, 64), (2, 4)))
    down_weights = bell_draw(key_of[14], (EXPERTS, HIDDEN_SIZE, D), (36 * HIDDEN_SIZE) ** -0.5, 0.0234375, ((0, 64), (1, 4)))
    return dict(filter_value=filter_value, filter_gate=filter_gate, filter_taps=filter_taps, filter_bias=filter_bias, norm_gain=norm_gain, norm_shift=norm_shift, out_weight=out_weight, out_bias=out_bias, expert_input=expert_input, expert_gain=expert_gain, route_experts=route_experts, route_weights=route_weights, gate_weights=gate_weights, up_weights=up_weights, down_weights=down_weights)


epsilon = 1e-06
clamp_limit = 7.0
swish_alpha = 1.702

def reference(filter_value, filter_gate, filter_taps, filter_bias, norm_gain, norm_shift, out_weight, out_bias, expert_input, expert_gain, route_experts, route_weights, gate_weights, up_weights, down_weights):
    gated = (filter_value.astype(jnp.float32) * jax.nn.sigmoid(filter_gate.astype(jnp.float32))).astype(jnp.bfloat16)
    length = gated.shape[0]
    padded = jnp.concatenate([jnp.zeros((TAPS - 1, CHANNELS), jnp.bfloat16), gated], 0)
    filtered = jnp.zeros((length, CHANNELS), jnp.float32)
    for offset in range(TAPS):
        filtered = filtered + filter_taps[offset] * padded[offset:offset + length].astype(jnp.float32)
    filtered = filtered + filter_bias
    average = lax.optimization_barrier(jnp.mean(filtered, 1, keepdims=True))
    centred = filtered - average
    variance = lax.optimization_barrier(jnp.mean(centred * centred, 1, keepdims=True))
    normed_filter = centred * lax.rsqrt(variance + epsilon) * norm_gain + norm_shift
    activated = jax.nn.silu(normed_filter).astype(jnp.bfloat16)
    mixer_out = (jnp.dot(activated, out_weight, preferred_element_type=jnp.float32) + out_bias).astype(jnp.bfloat16)
    token_values = expert_input.astype(jnp.float32)
    normed = (token_values * lax.rsqrt(lax.optimization_barrier(jnp.mean(token_values * token_values, 1, keepdims=True)) + epsilon) * expert_gain).astype(jnp.bfloat16)
    blocked = route_experts.reshape(N_EP, ROUTE_DEV * TOPK)
    onehot = (blocked[:, :, None] == jnp.arange(EXPERTS, dtype=jnp.int32)[None, None, :]).astype(jnp.int32)
    earlier = jnp.cumsum(onehot, 1) - onehot
    slot = lax.optimization_barrier(jnp.sum(earlier * onehot, 2)).astype(jnp.int32)
    row_slot = (jnp.arange(N_EP, dtype=jnp.int32)[:, None] * CAPACITY + slot).reshape(-1).astype(jnp.int32)
    flat_ids = route_experts.reshape(-1).astype(jnp.int32)
    copies = jnp.repeat(normed, TOPK, axis=0)
    buffer = jnp.zeros((EXPERTS, N_EP * CAPACITY, D), jnp.bfloat16).at[flat_ids, row_slot].set(copies)

    def expert_rows(operands):
        rows_in, gate_matrix, up_matrix, down_matrix = operands
        gate_pre = jnp.dot(rows_in, gate_matrix, preferred_element_type=jnp.float32)
        up_pre = jnp.dot(rows_in, up_matrix, preferred_element_type=jnp.float32)
        gate_held = jnp.minimum(gate_pre, clamp_limit)
        up_held = jnp.clip(up_pre, -clamp_limit, clamp_limit)
        hidden = (gate_held * jax.nn.sigmoid(swish_alpha * gate_held) * (up_held + 1.0)).astype(jnp.bfloat16)
        shards = hidden.reshape(-1, N_TP, HIDDEN_SIZE // N_TP).astype(jnp.float32)
        down_shards = down_matrix.reshape(N_TP, HIDDEN_SIZE // N_TP, D).astype(jnp.float32)
        partial_value = jnp.einsum('rpf,pfd->prd', shards, down_shards).astype(jnp.bfloat16)
        partial_value = lax.optimization_barrier(partial_value)
        return lax.optimization_barrier(jnp.sum(partial_value.astype(jnp.float32), 0)).astype(jnp.bfloat16)
    results = lax.map(expert_rows, (buffer, gate_weights, up_weights, down_weights))
    picked = results[flat_ids, row_slot].astype(jnp.float32).reshape(-1, TOPK, D)
    expert_out = lax.optimization_barrier(jnp.sum(picked * route_weights[:, :, None], 1)).astype(jnp.bfloat16)
    return (mixer_out, expert_out)
```

```python
import functools

import jax
import jax.numpy as jnp
from jax import lax
from jax.experimental import pallas as pl
from jax.experimental.pallas import tpu as pltpu
from jax.sharding import PartitionSpec as P

MESH = pl.DeviceIdType.MESH
BF16, F32, I32 = jnp.bfloat16, jnp.float32, jnp.int32

EPS = 1e-06
LIMIT = 7.0
ALPHA = 1.702

NZ = 8
PLANE = 8
NEP = 64
NTP = 4
SLOTS = 16
ROWS = PLANE * SLOTS
TOKENS = 256
WIDTH = 512
HALF = ROWS // 2
ORDER = (0, 1, -2, 2, -3, 3, 4, -1)
TAPS = 31
CHANNELS = 1024
TILE = 64


def copy_to(src, dst, send, recv, device):
    return pltpu.make_async_remote_copy(
        src_ref=src, dst_ref=dst, send_sem=send, recv_sem=recv, device_id=device, device_id_type=MESH
    )


def travel(group):
    value = jnp.int32(ORDER[0])
    for index, by in enumerate(ORDER):
        value = jnp.where(group == index, jnp.int32(by), value)
    return value


def kernel(
    value_ref, gate_ref, taps_ref, fbias_ref, ngain_ref, nshift_ref, ow_hbm, obias_ref,
    xin_ref, egain_ref, routes_ref, rweights_ref, wg_hbm, wu_hbm, wd_hbm,
    mixer_ref, out_ref,
    rm, tk, pick, nb, outgoing, rows_in, wg, wu, wd, ow, parts, first_in, second_out, second_in,
    summed, ret, halo_out, halo_in, gbuf, filt, act,
    load_sem, disp_send, disp_recv, ag_send, ag_recv, fwd_send, fwd_recv,
    rs1_send, rs1_recv, rs2_send, rs2_recv, ret_send, ret_recv, halo_send, halo_recv,
):
    me = lax.axis_index("ep")
    y = lax.axis_index("tp")
    z, own = me // PLANE, me % PLANE
    right, left = (y + 1) % NTP, (y + NTP - 1) % NTP
    line = me * NTP + y
    after = (line + 1) % (NEP * NTP)
    to_right, to_left = {"ep": me, "tp": right}, {"ep": me, "tp": left}
    to_after = {"ep": after // NTP, "tp": after % NTP}

    loads = []
    for k, shift in enumerate((0, 3, 1, 2)):
        at = pl.ds(pl.multiple_of((y + shift) % NTP * WIDTH, WIDTH), WIDTH)
        loads.append(pltpu.make_async_copy(wg_hbm.at[0, at, :], wg.at[k], load_sem.at[k]))
        loads.append(pltpu.make_async_copy(wu_hbm.at[0, at, :], wu.at[k], load_sem.at[4 + k]))
    for k, shift in enumerate((0, 1, 3, 2)):
        at = pl.ds(pl.multiple_of((y + shift) % NTP * WIDTH, WIDTH), WIDTH)
        loads.append(pltpu.make_async_copy(wd_hbm.at[0, :, at], wd.at[k], load_sem.at[8 + k]))
    loads.append(pltpu.make_async_copy(ow_hbm, ow, load_sem.at[12]))
    for load in loads:
        load.start()

    routes = routes_ref[...]
    expert = lax.broadcasted_iota(I32, (NEP, TOKENS), 0)
    named0 = routes[0:1, :] == expert
    named1 = routes[1:2, :] == expert
    named = jnp.logical_or(named0, named1)
    earlier = (
        lax.broadcasted_iota(I32, (TOKENS, TOKENS), 0) < lax.broadcasted_iota(I32, (TOKENS, TOKENS), 1)
    ).astype(F32).astype(BF16)
    rank = jnp.dot(named.astype(F32).astype(BF16), earlier, preferred_element_type=F32)
    rm[...] = jnp.where(named, rank, -1.0).astype(BF16)
    for k, hit in enumerate((named0, named1)):
        weight = jnp.broadcast_to(rweights_ref[k : k + 1, :], (NEP, TOKENS))
        tk[k] = jnp.concatenate([jnp.where(hit, rank, -1.0), weight], 0).T

    columns = pl.ds(pl.multiple_of(y * WIDTH, WIDTH), WIDTH)

    def normed(i, carry):
        at = pl.ds(pl.multiple_of(i * 16, 16), 16)
        tokens = xin_ref[at, :].astype(F32)
        scale = lax.rsqrt(jnp.mean(tokens * tokens, 1, keepdims=True) + EPS)
        nb[at, :] = (xin_ref[at, columns].astype(F32) * scale * egain_ref[0:1, columns]).astype(BF16)
        return carry

    lax.fori_loop(0, TOKENS // 16, normed, 0)

    row = lax.broadcasted_iota(I32, (ROWS, NEP), 0)
    col = lax.broadcasted_iota(I32, (ROWS, NEP), 1)
    slot_row = (lax.broadcasted_iota(I32, (ROWS, TOKENS), 0) % SLOTS).astype(F32)

    def place(group):
        target = (z + travel(group) + NZ) % NZ
        spread = (row // SLOTS + target * PLANE == col).astype(F32).astype(BF16)
        ranks = jnp.dot(spread, rm[...], preferred_element_type=F32)
        chosen = (ranks == slot_row).astype(F32).astype(BF16)
        outgoing[group] = jnp.dot(chosen, nb[...], preferred_element_type=F32).astype(BF16)

    def dispatch(group):
        target = (z + travel(group) + NZ) % NZ

        def one(q, carry):
            index = (own + q) % PLANE
            there = target * PLANE + index
            at = pl.ds(pl.multiple_of(index * SLOTS, SLOTS), SLOTS)
            mine = pl.ds(pl.multiple_of(own * SLOTS, SLOTS), SLOTS)

            @pl.when(there != me)
            def _():
                copy_to(
                    outgoing.at[group, at, :], rows_in.at[0, group, mine, :], disp_send, disp_recv.at[group],
                    {"ep": there, "tp": y},
                ).start()

            @pl.when(there == me)
            def _():
                rows_in[0, group, mine, :] = outgoing[group, mine, :]

            return carry

        lax.fori_loop(0, PLANE, one, 0)

    def place_and_send(group, carry):
        @pl.when(group < NZ)
        def _():
            place(group)

        @pl.when(group > 0)
        def _():
            dispatch(group - 1)

        return carry

    lax.fori_loop(0, NZ + 1, place_and_send, 0)

    def gated(i, carry):
        at = pl.ds(pl.multiple_of(i * 16, 16), 16)
        product = (value_ref[at, :].astype(F32) * jax.nn.sigmoid(gate_ref[at, :].astype(F32))).astype(BF16)
        gbuf[pl.ds(pl.multiple_of(i * 16 + 32, 16), 16), :] = product.astype(F32)

        @pl.when(i >= TOKENS // 16 - 2)
        def _():
            halo_out[pl.ds(pl.multiple_of(i * 16 - (TOKENS - 32), 16), 16), :] = product

        return carry

    lax.fori_loop(0, TOKENS // 16, gated, 0)
    halo = copy_to(halo_out, halo_in, halo_send, halo_recv, to_after)
    halo.start()

    def conv(tile):
        def lanes(block, carry):
            at = pl.ds(pl.multiple_of(block * 128, 128), 128)
            window = gbuf[pl.ds(pl.multiple_of(tile * TILE, TILE), TILE + 32), at]
            total = jnp.broadcast_to(fbias_ref[0:1, at], (TILE, 128))
            for r in range(8):
                moved = window if r == 0 else pltpu.roll(window, TILE + 32 - r, 0)
                for q in range(5):
                    j = 8 * q + r - 2
                    if 0 <= j < TAPS:
                        total = total + taps_ref[j : j + 1, at] * moved[8 * q : 8 * q + TILE]
            filt[:, at] = total
            return carry

        lax.fori_loop(0, CHANNELS // 128, lanes, 0)

        def norm(i, carry):
            at = pl.ds(pl.multiple_of(i * 16, 16), 16)
            rows = filt[at, :]
            centred = rows - jnp.mean(rows, 1, keepdims=True)
            variance = jnp.mean(centred * centred, 1, keepdims=True)
            out = centred * lax.rsqrt(variance + EPS) * ngain_ref[0:1, :] + nshift_ref[0:1, :]
            act[pl.ds(pl.multiple_of(tile * TILE + i * 16, 16), 16), :] = (out * jax.nn.sigmoid(out)).astype(BF16)
            return carry

        lax.fori_loop(0, TILE // 16, norm, 0)

    def project(chunk):
        at = pl.ds(pl.multiple_of(chunk * 512, 512), 512)
        out = jnp.dot(act[...], ow[:, at], preferred_element_type=F32) + obias_ref[0:1, at]
        mixer_ref[:, at] = out.astype(BF16)

    def gather_own(g):
        @pl.when(g == 0)
        def _():
            some = rows_in.at[0, 0, pl.ds(0, ROWS - SLOTS), :]
            copy_to(some, some, disp_send, disp_recv.at[0], to_right).wait_recv()

        @pl.when(g > 0)
        def _():
            every = rows_in.at[0, g]
            copy_to(every, every, disp_send, disp_recv.at[g], to_right).wait_recv()

        copy_to(rows_in.at[0, g], rows_in.at[1, g], ag_send, ag_recv.at[0, g], to_right).start()
        copy_to(rows_in.at[0, g], rows_in.at[2, g], ag_send, ag_recv.at[1, g], to_left).start()

    top, low = pl.ds(0, HALF), pl.ds(HALF, HALF)

    def gather_on(g):
        copy_to(rows_in.at[0, g], rows_in.at[1, g], ag_send, ag_recv.at[0, g], to_right).wait_recv()
        copy_to(rows_in.at[1, g, top, :], rows_in.at[3, g, top, :], fwd_send, fwd_recv.at[g], to_right).start()
        copy_to(rows_in.at[0, g], rows_in.at[2, g], ag_send, ag_recv.at[1, g], to_left).wait_recv()
        copy_to(rows_in.at[2, g, low, :], rows_in.at[3, g, low, :], fwd_send, fwd_recv.at[g], to_left).start()

    def experts(g):
        whole = rows_in.at[3, g]
        copy_to(whole, whole, fwd_send, fwd_recv.at[g], to_right).wait_recv()
        gate_pre = jnp.zeros((ROWS, WIDTH), F32)
        up_pre = jnp.zeros((ROWS, WIDTH), F32)
        for k in range(NTP):
            block = rows_in[k, g]
            gate_pre = gate_pre + jnp.dot(block, wg[k], preferred_element_type=F32)
            up_pre = up_pre + jnp.dot(block, wu[k], preferred_element_type=F32)
        gate_held = jnp.minimum(gate_pre, LIMIT)
        up_held = jnp.clip(up_pre, -LIMIT, LIMIT)
        hidden = (gate_held * jax.nn.sigmoid(ALPHA * gate_held) * (up_held + 1.0)).astype(BF16)
        for k in (3, 1, 2, 0):
            parts[k, g] = jnp.dot(hidden, wd[k], preferred_element_type=F32).astype(BF16)
        copy_to(parts.at[3, g, top, :], first_in.at[0, g], rs1_send, rs1_recv.at[0, g], to_right).start()
        copy_to(parts.at[3, g, low, :], first_in.at[1, g], rs1_send, rs1_recv.at[1, g], to_left).start()

    def reduce_on(g):
        copy_to(parts.at[3, g, top, :], first_in.at[0, g], rs1_send, rs1_recv.at[0, g], to_right).wait_recv()
        second_out[0, g, top, :] = (
            parts[1, g, top, :].astype(F32) + first_in[0, g].astype(F32)
        ).astype(BF16)
        second_out[0, g, low, :] = parts[1, g, low, :]
        copy_to(second_out.at[0, g], second_in.at[0, g], rs2_send, rs2_recv.at[0, g], to_right).start()
        copy_to(parts.at[3, g, low, :], first_in.at[1, g], rs1_send, rs1_recv.at[1, g], to_left).wait_recv()
        second_out[1, g, top, :] = parts[2, g, top, :]
        second_out[1, g, low, :] = (
            parts[2, g, low, :].astype(F32) + first_in[1, g].astype(F32)
        ).astype(BF16)
        copy_to(second_out.at[1, g], second_in.at[1, g], rs2_send, rs2_recv.at[1, g], to_left).start()

    def send_back(g):
        copy_to(second_out.at[0, g], second_in.at[0, g], rs2_send, rs2_recv.at[0, g], to_right).wait_recv()
        copy_to(second_out.at[1, g], second_in.at[1, g], rs2_send, rs2_recv.at[1, g], to_left).wait_recv()
        total = parts[0, g].astype(F32) + second_in[0, g].astype(F32) + second_in[1, g].astype(F32)
        summed[g] = total.astype(BF16)
        source = (z - travel(g) + NZ) % NZ
        mine = pl.ds(pl.multiple_of(me * SLOTS, SLOTS), SLOTS)

        def one(q, carry):
            index = (own + q) % PLANE
            there = source * PLANE + index
            at = pl.ds(pl.multiple_of(index * SLOTS, SLOTS), SLOTS)

            @pl.when(there != me)
            def _():
                copy_to(
                    summed.at[g, at, :], ret.at[mine, :], ret_send, ret_recv, {"ep": there, "tp": y}
                ).start()

            @pl.when(there == me)
            def _():
                ret[mine, :] = summed[g, at, :]

            return carry

        lax.fori_loop(0, PLANE, one, 0)

    def picks():
        lane = lax.broadcasted_iota(I32, (NEP, NEP * SLOTS), 1)
        spread = (lane // SLOTS == lax.broadcasted_iota(I32, (NEP, NEP * SLOTS), 0)).astype(F32).astype(BF16)
        slot = (lax.broadcasted_iota(I32, (TOKENS, NEP * SLOTS), 1) % SLOTS).astype(F32)
        for k in range(2):
            ranks = jnp.dot(tk[k][:, 0:NEP].astype(BF16), spread, preferred_element_type=F32)
            pick[k] = (ranks == slot).astype(F32).astype(BF16)

    def step(t, carry):
        @pl.when(t < NZ)
        def _():
            gather_own(t)

        @pl.when(jnp.logical_and(t >= 1, t < NZ + 1))
        def _():
            gather_on(t - 1)

        @pl.when(t >= 4)
        def _():
            send_back(t - 4)

        @pl.when(jnp.logical_and(t >= 3, t < NZ + 3))
        def _():
            reduce_on(t - 3)

        @pl.when(t == 2)
        def _():
            for load in loads[:12]:
                load.wait()

        @pl.when(jnp.logical_and(t >= 2, t < NZ + 2))
        def _():
            experts(t - 2)

        @pl.when(t == 0)
        def _():
            halo.wait()
            gbuf[0:32, :] = jnp.where(line == 0, 0.0, halo_in[...].astype(F32))

        @pl.when(t < 4)
        def _():
            conv(t)

        @pl.when(t == 4)
        def _():
            loads[12].wait()

        @pl.when(jnp.logical_and(t >= 4, t < 8))
        def _():
            project(t - 4)

        @pl.when(t == 8)
        def _():
            picks()

        return carry

    lax.fori_loop(0, NZ + 4, step, 0)

    but_one = ret.at[pl.ds(0, (NEP - 1) * SLOTS), :]
    copy_to(but_one, but_one, ret_send, ret_recv, to_right).wait_recv()
    expert_out = jnp.zeros((TOKENS, WIDTH), F32)
    for k in range(2):
        picked = jnp.dot(pick[k], ret[...], preferred_element_type=F32)
        expert_out = expert_out + picked * tk[k][:, NEP : NEP + 1]
    out_ref[...] = expert_out.astype(BF16)

    copy_to(but_one, but_one, disp_send, ret_recv, to_right).wait_send()
    copy_to(but_one, but_one, ret_send, ret_recv, to_right).wait_send()
    copy_to(second_in, second_in, ag_send, ret_recv, to_right).wait_send()
    copy_to(second_in, second_in, rs2_send, ret_recv, to_right).wait_send()
    copy_to(first_in, first_in, fwd_send, ret_recv, to_right).wait_send()
    copy_to(first_in, first_in, rs1_send, ret_recv, to_right).wait_send()


def local(
    filter_value, filter_gate, filter_taps, filter_bias, norm_gain, norm_shift, out_weight, out_bias,
    expert_input, expert_gain, route_experts, route_weights, gate_weights, up_weights, down_weights,
):
    vmem = pl.BlockSpec(memory_space=pltpu.VMEM)
    hbm = pl.BlockSpec(memory_space=pl.ANY)
    dma = pltpu.SemaphoreType.DMA
    return pl.pallas_call(
        kernel,
        out_shape=(
            jax.ShapeDtypeStruct((TOKENS, 2048), BF16),
            jax.ShapeDtypeStruct((TOKENS, WIDTH), BF16),
        ),
        in_specs=[vmem] * 6 + [hbm] + [vmem] * 5 + [hbm] * 3,
        out_specs=(vmem, vmem),
        scratch_shapes=[
            pltpu.VMEM((NEP, TOKENS), BF16),
            pltpu.VMEM((2, TOKENS, 2 * NEP), F32),
            pltpu.VMEM((2, TOKENS, NEP * SLOTS), BF16),
            pltpu.VMEM((TOKENS, WIDTH), BF16),
            pltpu.VMEM((NZ, ROWS, WIDTH), BF16),
            pltpu.VMEM((NTP, NZ, ROWS, WIDTH), BF16),
            pltpu.VMEM((NTP, WIDTH, WIDTH), BF16),
            pltpu.VMEM((NTP, WIDTH, WIDTH), BF16),
            pltpu.VMEM((NTP, WIDTH, WIDTH), BF16),
            pltpu.VMEM((CHANNELS, 2048), BF16),
            pltpu.VMEM((NTP, NZ, ROWS, WIDTH), BF16),
            pltpu.VMEM((2, NZ, HALF, WIDTH), BF16),
            pltpu.VMEM((2, NZ, ROWS, WIDTH), BF16),
            pltpu.VMEM((2, NZ, ROWS, WIDTH), BF16),
            pltpu.VMEM((NZ, ROWS, WIDTH), BF16),
            pltpu.VMEM((NEP * SLOTS, WIDTH), BF16),
            pltpu.VMEM((32, CHANNELS), BF16),
            pltpu.VMEM((32, CHANNELS), BF16),
            pltpu.VMEM((TOKENS + 32, CHANNELS), F32),
            pltpu.VMEM((TILE, CHANNELS), F32),
            pltpu.VMEM((TOKENS, CHANNELS), BF16),
            dma((13,)),
            dma, dma((NZ,)), dma, dma((2, NZ)), dma, dma((NZ,)),
            dma, dma((2, NZ)), dma, dma((2, NZ)), dma, dma, dma, dma,
        ],
        compiler_params=pltpu.CompilerParams(has_side_effects=True, vmem_limit_bytes=56 * 1024 * 1024),
        name="filter_and_experts",
    )(
        filter_value, filter_gate, filter_taps, filter_bias[None], norm_gain[None], norm_shift[None],
        out_weight, out_bias[None], expert_input, expert_gain[None], route_experts.T, route_weights.T,
        gate_weights, up_weights, down_weights,
    )


def solution(mesh):
    in_specs = (
        P(("ep", "tp"), None),
        P(("ep", "tp"), None),
        P(),
        P(),
        P(),
        P(),
        P(),
        P(),
        P("ep", None),
        P(),
        P("ep", None),
        P("ep", None),
        P("ep", None, "tp"),
        P("ep", None, "tp"),
        P("ep", "tp", None),
    )
    out_specs = (P(("ep", "tp"), None), P("ep", "tp"))
    return jax.shard_map(local, mesh=mesh, in_specs=in_specs, out_specs=out_specs, check_vma=False)
```

```python
import functools

import jax
import jax.numpy as jnp
from jax import lax
from jax.experimental import pallas as pl
from jax.experimental.pallas import tpu as pltpu
from jax.sharding import PartitionSpec as P

MESH = pl.DeviceIdType.MESH
BF16, F32, I32 = jnp.bfloat16, jnp.float32, jnp.int32

EPS = 1e-06
LIMIT = 7.0
ALPHA = 1.702

NZ = 8
PLANE = 8
NEP = 64
NTP = 4
SLOTS = 16
ROWS = PLANE * SLOTS
TOKENS = 256
WIDTH = 512
HALF = ROWS // 2
ORDER = (0, 2, -2, 4, 3, -3, 1, -1)
DIRECT = tuple(by in (0, 1, -1) for by in ORDER)
SCHEDULE = (
    "F3 F2 F1 W0",
    "C0 A1 A2 F0",
    "P0 P1 P2 D0",
    "P3 G0 B1 A3",
    "B2 E0 C1 A4",
    "A5 B3 C2 D1",
    "B4 B5 C6 C3",
    "C7 D2 E1 C4",
    "C5 D6 D3 D7",
    "E2 D4 D5 E6",
    "E3 E7 E4 E5",
)
OPS = tuple(("ABCDEFPGW".index(word[0]), int(word[1:])) for line in SCHEDULE for word in line.split())
GATHERED = NZ - sum(DIRECT)
TAPS = 31
CHANNELS = 1024
TILE = 64


def copy_to(src, dst, send, recv, device):
    return pltpu.make_async_remote_copy(
        src_ref=src, dst_ref=dst, send_sem=send, recv_sem=recv, device_id=device, device_id_type=MESH
    )


def lookup(table, index):
    value = jnp.int32(table[0])
    for at, entry in enumerate(table):
        if at and entry != table[0]:
            value = jnp.where(index == at, jnp.int32(entry), value)
    return value


def is_direct(group):
    value = jnp.bool_(False)
    for index, direct in enumerate(DIRECT):
        if direct:
            value = jnp.logical_or(value, group == index)
    return value


def kernel(
    value_hbm, gate_hbm, taps_hbm, fbias_hbm, ngain_hbm, nshift_hbm, ow_hbm, obias_hbm,
    xin_hbm, egain_hbm, routes_hbm, rweights_hbm, wg_hbm, wu_hbm, wd_hbm,
    mixer_ref, out_ref,
    value_ref, gate_ref, taps_ref, fbias_ref, ngain_ref, nshift_ref, obias_ref,
    xin_ref, egain_ref, routes_ref, rweights_ref,
    rm, tk, pick, nb, outgoing, rows_in, wg, wu, wd, ow, parts, first_in, second_out, second_in,
    summed, ret, halo_out, halo_in, gbuf, filt, act,
    early_sem, load_sem, disp_send, disp_recv, ag_send, ag_recv, fwd_send, fwd_recv,
    rs1_send, rs1_recv, rs2_send, rs2_recv, ret_send, ret_recv, halo_send, halo_recv,
):
    me = lax.axis_index("ep")
    y = lax.axis_index("tp")
    z, own = me // PLANE, me % PLANE
    right, left = (y + 1) % NTP, (y + NTP - 1) % NTP
    line = me * NTP + y
    after = (line + 1) % (NEP * NTP)
    to_right, to_left = {"ep": me, "tp": right}, {"ep": me, "tp": left}
    to_after = {"ep": after // NTP, "tp": after % NTP}

    early = [
        pltpu.make_async_copy(src, dst, early_sem.at[index])
        for index, (src, dst) in enumerate((
            (routes_hbm, routes_ref), (rweights_hbm, rweights_ref), (xin_hbm, xin_ref), (egain_hbm, egain_ref),
            (value_hbm, value_ref), (gate_hbm, gate_ref), (taps_hbm, taps_ref), (fbias_hbm, fbias_ref),
            (ngain_hbm, ngain_ref), (nshift_hbm, nshift_ref), (obias_hbm, obias_ref),
        ))
    ]
    for load in early:
        load.start()

    before = (line + NEP * NTP - 1) % (NEP * NTP)
    barrier = pltpu.get_barrier_semaphore()

    def greet(i, carry):
        peer = {"ep": (me + i) % NEP, "tp": y}
        pl.semaphore_signal(barrier, inc=1, device_id=peer, device_id_type=MESH)
        return carry

    lax.fori_loop(1, NEP, greet, 0)
    for peer in (to_right, to_left, to_after, {"ep": before // NTP, "tp": before % NTP}):
        pl.semaphore_signal(barrier, inc=1, device_id=peer, device_id_type=MESH)

    loads = []
    for k, shift in enumerate((0, 3, 1, 2)):
        at = pl.ds(pl.multiple_of((y + shift) % NTP * WIDTH, WIDTH), WIDTH)
        loads.append(pltpu.make_async_copy(wg_hbm.at[0, at, :], wg.at[k], load_sem.at[k]))
        loads.append(pltpu.make_async_copy(wu_hbm.at[0, at, :], wu.at[k], load_sem.at[4 + k]))
    for k, shift in enumerate((0, 1, 3, 2)):
        at = pl.ds(pl.multiple_of((y + shift) % NTP * WIDTH, WIDTH), WIDTH)
        loads.append(pltpu.make_async_copy(wd_hbm.at[0, :, at], wd.at[k], load_sem.at[8 + k]))
    loads.append(pltpu.make_async_copy(ow_hbm, ow, load_sem.at[12]))
    for load in loads:
        load.start()

    for load in early[:2]:
        load.wait()
    routes = routes_ref[...]
    expert = lax.broadcasted_iota(I32, (NEP, TOKENS), 0)
    named0 = routes[0:1, :] == expert
    named1 = routes[1:2, :] == expert
    named = jnp.logical_or(named0, named1)
    earlier = (
        lax.broadcasted_iota(I32, (TOKENS, TOKENS), 0) < lax.broadcasted_iota(I32, (TOKENS, TOKENS), 1)
    ).astype(F32).astype(BF16)
    rank = jnp.dot(named.astype(F32).astype(BF16), earlier, preferred_element_type=F32)
    rm[...] = jnp.where(named, rank, -1.0).astype(BF16)
    for k, hit in enumerate((named0, named1)):
        weight = jnp.broadcast_to(rweights_ref[k : k + 1, :], (NEP, TOKENS))
        tk[k] = jnp.concatenate([jnp.where(hit, rank, -1.0), weight], 0).T

    columns = [pl.ds(pl.multiple_of((y + shift) % NTP * WIDTH, WIDTH), WIDTH) for shift in (0, 3, 1, 2)]

    def normed(i, carry):
        at = pl.ds(pl.multiple_of(i * 16, 16), 16)
        tokens = xin_ref[at, :].astype(F32)
        scale = lax.rsqrt(jnp.mean(tokens * tokens, 1, keepdims=True) + EPS)
        for k in range(NTP):
            nb[k, at, :] = (xin_ref[at, columns[k]].astype(F32) * scale * egain_ref[0:1, columns[k]]).astype(BF16)
        return carry

    for load in early[2:4]:
        load.wait()
    lax.fori_loop(0, TOKENS // 16, normed, 0)

    row = lax.broadcasted_iota(I32, (ROWS, NEP), 0)
    col = lax.broadcasted_iota(I32, (ROWS, NEP), 1)
    slot_row = (lax.broadcasted_iota(I32, (ROWS, TOKENS), 0) % SLOTS).astype(F32)

    def place(group):
        target = (z + lookup(ORDER, group) + NZ) % NZ
        spread = (row // SLOTS + target * PLANE == col).astype(F32).astype(BF16)
        ranks = jnp.dot(spread, rm[...], preferred_element_type=F32)
        chosen = (ranks == slot_row).astype(F32).astype(BF16)
        outgoing[0, group] = jnp.dot(chosen, nb[0], preferred_element_type=F32).astype(BF16)

        @pl.when(is_direct(group))
        def _():
            for k in range(1, NTP):
                outgoing[k, group] = jnp.dot(chosen, nb[k], preferred_element_type=F32).astype(BF16)

    def dispatch(group):
        target = (z + lookup(ORDER, group) + NZ) % NZ

        def one(q, carry):
            index = (own + q) % PLANE
            there = target * PLANE + index
            at = pl.ds(pl.multiple_of(index * SLOTS, SLOTS), SLOTS)
            mine = pl.ds(pl.multiple_of(own * SLOTS, SLOTS), SLOTS)

            @pl.when(jnp.logical_not(is_direct(group)))
            def _():
                copy_to(
                    outgoing.at[0, group, at, :], rows_in.at[0, group, mine, :],
                    disp_send.at[group], disp_recv.at[group], {"ep": there, "tp": y},
                ).start()

            @pl.when(jnp.logical_and(is_direct(group), there != me))
            def _():
                copy_to(
                    outgoing.at[:, group, at, :], rows_in.at[:, group, mine, :],
                    disp_send.at[group], disp_recv.at[group], {"ep": there, "tp": y},
                ).start()

            @pl.when(there == me)
            def _():
                for k in range(NTP):
                    rows_in[k, group, mine, :] = outgoing[k, group, mine, :]

            return carry

        lax.fori_loop(0, PLANE, one, 0)

    def place_and_send(group, carry):
        @pl.when(group < NZ)
        def _():
            place(group)

        @pl.when(group > 0)
        def _():
            dispatch(group - 1)

        return carry

    def gated(i, carry):
        at = pl.ds(pl.multiple_of(i * 16, 16), 16)
        product = (value_ref[at, :].astype(F32) * jax.nn.sigmoid(gate_ref[at, :].astype(F32))).astype(BF16)
        gbuf[pl.ds(pl.multiple_of(i * 16 + 32, 16), 16), :] = product.astype(F32)

        @pl.when(i >= TOKENS // 16 - 2)
        def _():
            halo_out[pl.ds(pl.multiple_of(i * 16 - (TOKENS - 32), 16), 16), :] = product

        return carry

    for load in early[4:]:
        load.wait()
    lax.fori_loop(TOKENS // 16 - 2, TOKENS // 16, gated, 0)
    place(0)
    pl.semaphore_wait(barrier, NEP - 1 + 4)
    halo = copy_to(halo_out, halo_in, halo_send, halo_recv, to_after)
    halo.start()
    lax.fori_loop(1, NZ + 1, place_and_send, 0)
    lax.fori_loop(0, TOKENS // 16 - 2, gated, 0)

    def conv(tile):
        def lanes(block, carry):
            at = pl.ds(pl.multiple_of(block * 128, 128), 128)
            window = gbuf[pl.ds(pl.multiple_of(tile * TILE, TILE), TILE + 32), at]
            total = jnp.broadcast_to(fbias_ref[0:1, at], (TILE, 128))
            for r in range(8):
                moved = window if r == 0 else pltpu.roll(window, TILE + 32 - r, 0)
                for q in range(5):
                    j = 8 * q + r - 2
                    if 0 <= j < TAPS:
                        total = total + taps_ref[j : j + 1, at] * moved[8 * q : 8 * q + TILE]
            filt[:, at] = total
            return carry

        lax.fori_loop(0, CHANNELS // 128, lanes, 0)

        def norm(i, carry):
            at = pl.ds(pl.multiple_of(i * 16, 16), 16)
            rows = filt[at, :]
            centred = rows - jnp.mean(rows, 1, keepdims=True)
            variance = jnp.mean(centred * centred, 1, keepdims=True)
            out = centred * lax.rsqrt(variance + EPS) * ngain_ref[0:1, :] + nshift_ref[0:1, :]
            act[pl.ds(pl.multiple_of(tile * TILE + i * 16, 16), 16), :] = (out * jax.nn.sigmoid(out)).astype(BF16)
            return carry

        lax.fori_loop(0, TILE // 16, norm, 0)

    def project(chunk):
        at = pl.ds(pl.multiple_of(chunk * 512, 512), 512)
        out = jnp.dot(act[...], ow[:, at], preferred_element_type=F32) + obias_ref[0:1, at]
        mixer_ref[:, at] = out.astype(BF16)

    def arrived(g):
        for group, by in enumerate(ORDER):
            every = rows_in.at[0, group]
            if DIRECT[group]:
                count = ROWS - SLOTS if by == 0 else ROWS
                every = rows_in.at[:, group, pl.ds(0, count), :]

            @pl.when(g == group)
            def _():
                copy_to(every, every, disp_send.at[group], disp_recv.at[group], to_right).wait_recv()

    def gather_own(g):
        arrived(g)
        copy_to(rows_in.at[0, g], rows_in.at[1, g], ag_send, ag_recv.at[0, g], to_right).start()
        copy_to(rows_in.at[0, g], rows_in.at[2, g], ag_send, ag_recv.at[1, g], to_left).start()

    top, low = pl.ds(0, HALF), pl.ds(HALF, HALF)

    def gather_on(g):
        copy_to(rows_in.at[0, g], rows_in.at[1, g], ag_send, ag_recv.at[0, g], to_right).wait_recv()
        copy_to(rows_in.at[1, g, top, :], rows_in.at[3, g, top, :], fwd_send, fwd_recv.at[g], to_right).start()
        copy_to(rows_in.at[0, g], rows_in.at[2, g], ag_send, ag_recv.at[1, g], to_left).wait_recv()
        copy_to(rows_in.at[2, g, low, :], rows_in.at[3, g, low, :], fwd_send, fwd_recv.at[g], to_left).start()

    def experts(g):
        whole = rows_in.at[3, g]

        @pl.when(is_direct(g))
        def _():
            arrived(g)

        @pl.when(jnp.logical_not(is_direct(g)))
        def _():
            copy_to(whole, whole, fwd_send, fwd_recv.at[g], to_right).wait_recv()

        gate_pre = jnp.zeros((ROWS, WIDTH), F32)
        up_pre = jnp.zeros((ROWS, WIDTH), F32)
        for k in range(NTP):
            block = rows_in[k, g]
            gate_pre = gate_pre + jnp.dot(block, wg[k], preferred_element_type=F32)
            up_pre = up_pre + jnp.dot(block, wu[k], preferred_element_type=F32)
        gate_held = jnp.minimum(gate_pre, LIMIT)
        up_held = jnp.clip(up_pre, -LIMIT, LIMIT)
        hidden = (gate_held * jax.nn.sigmoid(ALPHA * gate_held) * (up_held + 1.0)).astype(BF16)
        for k in (3, 1, 2, 0):
            parts[k, g] = jnp.dot(hidden, wd[k], preferred_element_type=F32).astype(BF16)
        copy_to(parts.at[3, g, top, :], first_in.at[0, g], rs1_send, rs1_recv.at[0, g], to_right).start()
        copy_to(parts.at[3, g, low, :], first_in.at[1, g], rs1_send, rs1_recv.at[1, g], to_left).start()

    def reduce_on(g):
        copy_to(parts.at[3, g, top, :], first_in.at[0, g], rs1_send, rs1_recv.at[0, g], to_right).wait_recv()
        second_out[0, g, top, :] = (
            parts[1, g, top, :].astype(F32) + first_in[0, g].astype(F32)
        ).astype(BF16)
        second_out[0, g, low, :] = parts[1, g, low, :]
        copy_to(second_out.at[0, g], second_in.at[0, g], rs2_send, rs2_recv.at[0, g], to_right).start()
        copy_to(parts.at[3, g, low, :], first_in.at[1, g], rs1_send, rs1_recv.at[1, g], to_left).wait_recv()
        second_out[1, g, top, :] = parts[2, g, top, :]
        second_out[1, g, low, :] = (
            parts[2, g, low, :].astype(F32) + first_in[1, g].astype(F32)
        ).astype(BF16)
        copy_to(second_out.at[1, g], second_in.at[1, g], rs2_send, rs2_recv.at[1, g], to_left).start()

    def send_back(g):
        copy_to(second_out.at[0, g], second_in.at[0, g], rs2_send, rs2_recv.at[0, g], to_right).wait_recv()
        copy_to(second_out.at[1, g], second_in.at[1, g], rs2_send, rs2_recv.at[1, g], to_left).wait_recv()
        total = parts[0, g].astype(F32) + second_in[0, g].astype(F32) + second_in[1, g].astype(F32)
        summed[g] = total.astype(BF16)
        source = (z - lookup(ORDER, g) + NZ) % NZ
        mine = pl.ds(pl.multiple_of(me * SLOTS, SLOTS), SLOTS)

        def one(q, carry):
            index = (own + q) % PLANE
            there = source * PLANE + index
            at = pl.ds(pl.multiple_of(index * SLOTS, SLOTS), SLOTS)

            @pl.when(there != me)
            def _():
                copy_to(
                    summed.at[g, at, :], ret.at[mine, :], ret_send, ret_recv, {"ep": there, "tp": y}
                ).start()

            @pl.when(there == me)
            def _():
                ret[mine, :] = summed[g, at, :]

            return carry

        lax.fori_loop(0, PLANE, one, 0)

    def picks(_):
        lane = lax.broadcasted_iota(I32, (NEP, NEP * SLOTS), 1)
        spread = (lane // SLOTS == lax.broadcasted_iota(I32, (NEP, NEP * SLOTS), 0)).astype(F32).astype(BF16)
        slot = (lax.broadcasted_iota(I32, (TOKENS, NEP * SLOTS), 1) % SLOTS).astype(F32)
        for k in range(2):
            ranks = jnp.dot(tk[k][:, 0:NEP].astype(BF16), spread, preferred_element_type=F32)
            pick[k] = (ranks == slot).astype(F32).astype(BF16)

    def loaded(_):
        for load in loads[:12]:
            load.wait()

    def filtered(tile):
        @pl.when(tile == 0)
        def _():
            halo.wait()
            gbuf[0:32, :] = jnp.where(line == 0, 0.0, halo_in[...].astype(F32))

        conv(tile)

    def projected(chunk):
        @pl.when(chunk == 0)
        def _():
            loads[12].wait()

        project(chunk)

    actions = (gather_own, gather_on, experts, reduce_on, send_back, filtered, projected, picks, loaded)

    def step(i, carry):
        code = lookup([op for op, _ in OPS], i)
        which = lookup([index for _, index in OPS], i)
        for number, action in enumerate(actions):

            @pl.when(code == number)
            def _():
                action(which)

        return carry

    lax.fori_loop(0, len(OPS), step, 0)

    but_one = ret.at[pl.ds(0, (NEP - 1) * SLOTS), :]
    copy_to(but_one, but_one, ret_send, ret_recv, to_right).wait_recv()
    expert_out = jnp.zeros((TOKENS, WIDTH), F32)
    for k in range(2):
        picked = jnp.dot(pick[k], ret[...], preferred_element_type=F32)
        expert_out = expert_out + picked * tk[k][:, NEP : NEP + 1]
    out_ref[...] = expert_out.astype(BF16)

    for group, by in enumerate(ORDER):
        every = rows_in.at[0, group]
        if DIRECT[group]:
            every = rows_in.at[:, group, pl.ds(0, ROWS - SLOTS if by == 0 else ROWS), :]
        copy_to(every, every, disp_send.at[group], ret_recv, to_right).wait_send()
    copy_to(but_one, but_one, ret_send, ret_recv, to_right).wait_send()
    some = second_in.at[:, pl.ds(0, GATHERED)]
    copy_to(some, some, ag_send, ret_recv, to_right).wait_send()
    copy_to(second_in, second_in, rs2_send, ret_recv, to_right).wait_send()
    some = first_in.at[:, pl.ds(0, GATHERED)]
    copy_to(some, some, fwd_send, ret_recv, to_right).wait_send()
    copy_to(first_in, first_in, rs1_send, ret_recv, to_right).wait_send()


def local(
    filter_value, filter_gate, filter_taps, filter_bias, norm_gain, norm_shift, out_weight, out_bias,
    expert_input, expert_gain, route_experts, route_weights, gate_weights, up_weights, down_weights,
):
    vmem = pl.BlockSpec(memory_space=pltpu.VMEM)
    hbm = pl.BlockSpec(memory_space=pltpu.HBM)
    dma = pltpu.SemaphoreType.DMA
    arguments = (
        filter_value, filter_gate, filter_taps, filter_bias[None], norm_gain[None], norm_shift[None],
        out_weight, out_bias[None], expert_input, expert_gain[None], route_experts.T, route_weights.T,
        gate_weights, up_weights, down_weights,
    )
    small = [argument for index, argument in enumerate(arguments[:12]) if index != 6]
    return pl.pallas_call(
        kernel,
        out_shape=(
            jax.ShapeDtypeStruct((TOKENS, 2048), BF16),
            jax.ShapeDtypeStruct((TOKENS, WIDTH), BF16),
        ),
        in_specs=[hbm] * len(arguments),
        out_specs=(vmem, vmem),
        scratch_shapes=[pltpu.VMEM(argument.shape, argument.dtype) for argument in small]
        + [
            pltpu.VMEM((NEP, TOKENS), BF16),
            pltpu.VMEM((2, TOKENS, 2 * NEP), F32),
            pltpu.VMEM((2, TOKENS, NEP * SLOTS), BF16),
            pltpu.VMEM((NTP, TOKENS, WIDTH), BF16),
            pltpu.VMEM((NTP, NZ, ROWS, WIDTH), BF16),
            pltpu.VMEM((NTP, NZ, ROWS, WIDTH), BF16),
            pltpu.VMEM((NTP, WIDTH, WIDTH), BF16),
            pltpu.VMEM((NTP, WIDTH, WIDTH), BF16),
            pltpu.VMEM((NTP, WIDTH, WIDTH), BF16),
            pltpu.VMEM((CHANNELS, 2048), BF16),
            pltpu.VMEM((NTP, NZ, ROWS, WIDTH), BF16),
            pltpu.VMEM((2, NZ, HALF, WIDTH), BF16),
            pltpu.VMEM((2, NZ, ROWS, WIDTH), BF16),
            pltpu.VMEM((2, NZ, ROWS, WIDTH), BF16),
            pltpu.VMEM((NZ, ROWS, WIDTH), BF16),
            pltpu.VMEM((NEP * SLOTS, WIDTH), BF16),
            pltpu.VMEM((32, CHANNELS), BF16),
            pltpu.VMEM((32, CHANNELS), BF16),
            pltpu.VMEM((TOKENS + 32, CHANNELS), F32),
            pltpu.VMEM((TILE, CHANNELS), F32),
            pltpu.VMEM((TOKENS, CHANNELS), BF16),
            dma((11,)), dma((13,)),
            dma((NZ,)), dma((NZ,)), dma, dma((2, NZ)), dma, dma((NZ,)),
            dma, dma((2, NZ)), dma, dma((2, NZ)), dma, dma, dma, dma,
        ],
        compiler_params=pltpu.CompilerParams(collective_id=0, has_side_effects=True, vmem_limit_bytes=46 * 1024 * 1024),
        name="filter_and_experts",
    )(*(pltpu.with_memory_space_constraint(argument, pltpu.HBM) for argument in arguments))


def solution(mesh):
    in_specs = (
        P(("ep", "tp"), None),
        P(("ep", "tp"), None),
        P(),
        P(),
        P(),
        P(),
        P(),
        P(),
        P("ep", None),
        P(),
        P("ep", None),
        P("ep", None),
        P("ep", None, "tp"),
        P("ep", None, "tp"),
        P("ep", "tp", None),
    )
    out_specs = (P(("ep", "tp"), None), P("ep", "tp"))
    return jax.shard_map(local, mesh=mesh, in_specs=in_specs, out_specs=out_specs, check_vma=False)
```

```python
import functools

import jax
import jax.numpy as jnp
from jax import lax
from jax.experimental import pallas as pl
from jax.experimental.pallas import tpu as pltpu
from jax.sharding import PartitionSpec as P

MESH = pl.DeviceIdType.MESH
BF16, F32, I32 = jnp.bfloat16, jnp.float32, jnp.int32

EPS = 1e-06
LIMIT = 7.0
ALPHA = 1.702

NZ = 8
NX = 4
PLANE = 8
NEP = 64
NTP = 4
SLOTS = 16
PLANE_ROWS = PLANE * SLOTS
TOKENS = 256
WIDTH = 512
AWAY = (0, 1, -1, 2, -2, 3, -3, 4)
DIRECT = (
    1, 2, 3, 4, 5, 6, 8,
)
SCHEDULE = (
    "S9 S11 S0 S1",
    "S12 F3 S10 F2",
    "F1 S13 A0 F0",
    "S14 A9 P0 P1",
    "P2 B0 A11 S7",
    "P3 G0 B9 A12",
    "W0 C0 S15 B11",
    "A10 S5 S3 B12",
    "A13 D0 A7 B10",
    "A14 S8 S6 B13",
    "A15 E0 B7 C5",
    "B14 C6 B15 D5",
    "S4 S2 R0 D6",
    "C7 E5 C4 C3",
    "E6 D7 D4 C2",
    "C1 D3 E7 E4",
    "D2 D1 R5 E3",
    "R6 E2 E1 R7",
    "R4 R3 R2 R1",
)
KINDS = "SABDERCFPGW"
STEPS = tuple(KINDS.index(word[0]) * 16 + int(word[1:]) for line in SCHEDULE for word in line.split())
WORDS = tuple(
    sum(step << 8 * at for at, step in enumerate(STEPS[first : first + 3])) for first in range(0, len(STEPS), 3)
)
ROWS = PLANE_ROWS
PART = ROWS // 2
QUARTER = PART // 2
IS_DIRECT = tuple(int(half in DIRECT) for half in range(2 * NZ))
GATHERED = 2 * NZ - len(DIRECT)
TAPS = 31
CHANNELS = 1024
TILE = 64


def copy_to(src, dst, send, recv, device):
    return pltpu.make_async_remote_copy(
        src_ref=src, dst_ref=dst, send_sem=send, recv_sem=recv, device_id=device, device_id_type=MESH
    )


def lookup(table, index):
    value = jnp.int32(table[0])
    for at, entry in enumerate(table):
        if at and entry != table[0]:
            value = jnp.where(index == at, jnp.int32(entry), value)
    return value


def is_direct(half):
    return lookup(IS_DIRECT, half) == 1


def kernel(
    value_hbm, gate_hbm, taps_hbm, fbias_hbm, ngain_hbm, nshift_hbm, ow_hbm, obias_hbm,
    xin_hbm, egain_hbm, routes_hbm, rweights_hbm, wg_hbm, wu_hbm, wd_hbm,
    mixer_ref, out_ref,
    value_ref, gate_ref, taps_ref, fbias_ref, ngain_ref, nshift_ref, obias_ref,
    xin_ref, egain_ref, routes_ref, rweights_ref,
    rm, tk, pick, nb, outgoing, rows_in, wg, wu, wd, ow, parts, first_in, second_out, second_in,
    summed, ret, total, halo_out, halo_in, gbuf, filt, act,
    early_sem, load_sem, disp_send, disp_recv, ag_send, ag_recv, fwd_send, fwd_recv,
    rs1_send, rs1_recv, rs2_send, rs2_recv, ret_send, ret_recv, halo_send, halo_recv,
):
    me = lax.axis_index("ep")
    y = lax.axis_index("tp")
    z, x, core = me // PLANE, me % PLANE // 2, me % 2
    right, left = (y + 1) % NTP, (y + NTP - 1) % NTP
    line = me * NTP + y
    after = (line + 1) % (NEP * NTP)
    to_right, to_left = {"ep": me, "tp": right}, {"ep": me, "tp": left}
    to_after = {"ep": after // NTP, "tp": after % NTP}

    early = [
        pltpu.make_async_copy(src, dst, early_sem.at[index])
        for index, (src, dst) in enumerate((
            (routes_hbm, routes_ref), (rweights_hbm, rweights_ref), (xin_hbm, xin_ref), (egain_hbm, egain_ref),
            (value_hbm, value_ref), (gate_hbm, gate_ref), (taps_hbm, taps_ref), (fbias_hbm, fbias_ref),
            (ngain_hbm, ngain_ref), (nshift_hbm, nshift_ref), (obias_hbm, obias_ref),
        ))
    ]
    for load in early[:4]:
        load.start()

    before = (line + NEP * NTP - 1) % (NEP * NTP)
    barrier = pltpu.get_barrier_semaphore()

    def greet(i, carry):
        peer = {"ep": (me + NEP // 2 + i) % NEP, "tp": y}
        pl.semaphore_signal(barrier, inc=1, device_id=peer, device_id_type=MESH)
        return carry

    lax.fori_loop(0, NEP // 2, greet, 0)
    lax.fori_loop(NEP // 2 + 1, NEP, greet, 0)
    for peer in (to_right, to_left, to_after, {"ep": before // NTP, "tp": before % NTP}):
        pl.semaphore_signal(barrier, inc=1, device_id=peer, device_id_type=MESH)

    for load in early[4:]:
        load.start()
    loads = []
    for k, shift in enumerate((0, 3, 1, 2)):
        at = pl.ds(pl.multiple_of((y + shift) % NTP * WIDTH, WIDTH), WIDTH)
        loads.append(pltpu.make_async_copy(wg_hbm.at[0, at, :], wg.at[k], load_sem.at[k]))
        loads.append(pltpu.make_async_copy(wu_hbm.at[0, at, :], wu.at[k], load_sem.at[4 + k]))
    for k, shift in enumerate((0, 1, 3, 2)):
        at = pl.ds(pl.multiple_of((y + shift) % NTP * WIDTH, WIDTH), WIDTH)
        loads.append(pltpu.make_async_copy(wd_hbm.at[0, :, at], wd.at[k], load_sem.at[8 + k]))
    loads.append(pltpu.make_async_copy(ow_hbm, ow, load_sem.at[12]))
    for load in loads:
        load.start()

    for load in early[:2]:
        load.wait()
    routes = routes_ref[...]
    expert = lax.broadcasted_iota(I32, (NEP, TOKENS), 0)
    named0 = routes[0:1, :] == expert
    named1 = routes[1:2, :] == expert
    named = jnp.logical_or(named0, named1)
    earlier = (
        lax.broadcasted_iota(I32, (TOKENS, TOKENS), 0) < lax.broadcasted_iota(I32, (TOKENS, TOKENS), 1)
    ).astype(F32).astype(BF16)
    rank = jnp.dot(named.astype(F32).astype(BF16), earlier, preferred_element_type=F32)
    rm[...] = jnp.where(named, rank, -1.0).astype(BF16)
    for k, hit in enumerate((named0, named1)):
        weight = jnp.broadcast_to(rweights_ref[k : k + 1, :], (NEP, TOKENS))
        tk[k] = jnp.concatenate([jnp.where(hit, rank, -1.0), weight], 0).T

    columns = [pl.ds(pl.multiple_of((y + shift) % NTP * WIDTH, WIDTH), WIDTH) for shift in (0, 3, 1, 2)]

    def normed(i, carry):
        at = pl.ds(pl.multiple_of(i * 16, 16), 16)
        tokens = xin_ref[at, :].astype(F32)
        scale = lax.rsqrt(jnp.mean(tokens * tokens, 1, keepdims=True) + EPS)
        for k in range(NTP):
            nb[k, at, :] = (xin_ref[at, columns[k]].astype(F32) * scale * egain_ref[0:1, columns[k]]).astype(BF16)
        return carry

    for load in early[2:4]:
        load.wait()
    lax.fori_loop(0, TOKENS // 16, normed, 0, unroll=4)

    row = lax.broadcasted_iota(I32, (PLANE_ROWS, NEP), 0)
    col = lax.broadcasted_iota(I32, (PLANE_ROWS, NEP), 1)
    slot_row = (lax.broadcasted_iota(I32, (PLANE_ROWS, TOKENS), 0) % SLOTS).astype(F32)

    def ahead(r):
        return (z + lookup(AWAY, r) + NZ) % NZ

    def place(r):
        spread = (row // SLOTS + ahead(r) * PLANE == col).astype(F32).astype(BF16)
        ranks = jnp.dot(spread, rm[...], preferred_element_type=F32)
        chosen = (ranks == slot_row).astype(F32).astype(BF16)
        for k in range(NTP if IS_DIRECT[2 * r] or IS_DIRECT[2 * r + 1] else 1):
            outgoing[k, r] = jnp.dot(chosen, nb[k], preferred_element_type=F32).astype(BF16)

    def dispatch(half):
        r, part = half // 2, half % 2
        direct = is_direct(half)
        for i in range(4):
            target = (x + part + 2 * (i // 2)) % NX * 2 + i % 2
            there = ahead(r) * PLANE + target
            at = pl.ds(pl.multiple_of(target * SLOTS, SLOTS), SLOTS)
            mine = pl.ds(pl.multiple_of(part * PART + (i // 2 * 2 + core) * SLOTS, SLOTS), SLOTS)

            @pl.when(jnp.logical_and(jnp.logical_not(direct), there != me))
            def _():
                copy_to(
                    outgoing.at[0, r, at, :], rows_in.at[0, r, mine, :],
                    disp_send.at[half], disp_recv.at[half], {"ep": there, "tp": y},
                ).start()

            @pl.when(jnp.logical_and(direct, there != me))
            def _():
                copy_to(
                    outgoing.at[:, r, at, :], rows_in.at[:, r, mine, :],
                    disp_send.at[half], disp_recv.at[half], {"ep": there, "tp": y},
                ).start()

            if i < 2:

                @pl.when(there == me)
                def _():
                    for k in range(NTP if IS_DIRECT[0] else 1):
                        rows_in[k, 0, mine, :] = outgoing[k, 0, at, :]

    def gated(i, carry):
        at = pl.ds(pl.multiple_of(i * 16, 16), 16)
        product = (value_ref[at, :].astype(F32) * jax.nn.sigmoid(gate_ref[at, :].astype(F32))).astype(BF16)
        gbuf[pl.ds(pl.multiple_of(i * 16 + 32, 16), 16), :] = product.astype(F32)

        @pl.when(i >= TOKENS // 16 - 2)
        def _():
            halo_out[pl.ds(pl.multiple_of(i * 16 - (TOKENS - 32), 16), 16), :] = product

        return carry

    for load in early[4:]:
        load.wait()
    lax.fori_loop(0, TOKENS // 16, gated, 0)
    for r in range(NZ):
        place(r)
    pl.semaphore_wait(barrier, NEP - 1 + 4)
    halo = copy_to(halo_out, halo_in, halo_send, halo_recv, to_after)
    halo.start()

    def conv(tile):
        def lanes(block, carry):
            at = pl.ds(pl.multiple_of(block * 128, 128), 128)
            window = gbuf[pl.ds(pl.multiple_of(tile * TILE, TILE), TILE + 32), at]
            value = jnp.broadcast_to(fbias_ref[0:1, at], (TILE, 128))
            for r in range(8):
                moved = window if r == 0 else pltpu.roll(window, TILE + 32 - r, 0)
                for q in range(5):
                    j = 8 * q + r - 2
                    if 0 <= j < TAPS:
                        value = value + taps_ref[j : j + 1, at] * moved[8 * q : 8 * q + TILE]
            filt[:, at] = value
            return carry

        lax.fori_loop(0, CHANNELS // 128, lanes, 0)

        def norm(i, carry):
            at = pl.ds(pl.multiple_of(i * 16, 16), 16)
            rows = filt[at, :]
            centred = rows - jnp.mean(rows, 1, keepdims=True)
            variance = jnp.mean(centred * centred, 1, keepdims=True)
            out = centred * lax.rsqrt(variance + EPS) * ngain_ref[0:1, :] + nshift_ref[0:1, :]
            act[pl.ds(pl.multiple_of(tile * TILE + i * 16, 16), 16), :] = (out * jax.nn.sigmoid(out)).astype(BF16)
            return carry

        lax.fori_loop(0, TILE // 16, norm, 0, unroll=True)

    def project(chunk):
        at = pl.ds(pl.multiple_of(chunk * 512, 512), 512)
        out = jnp.dot(act[...], ow[:, at], preferred_element_type=F32) + obias_ref[0:1, at]
        mixer_ref[:, at] = out.astype(BF16)

    def rows_of(half):
        return pl.ds(pl.multiple_of(half % 2 * PART, PART), PART)

    def arrived(half):
        r, direct, other = half // 2, is_direct(half), half != 0

        @pl.when(jnp.logical_and(jnp.logical_not(direct), other))
        def _():
            every = rows_in.at[0, r, rows_of(half), :]
            copy_to(every, every, disp_send.at[half], disp_recv.at[half], to_right).wait_recv()

        @pl.when(jnp.logical_and(direct, other))
        def _():
            every = rows_in.at[:, r, rows_of(half), :]
            copy_to(every, every, disp_send.at[half], disp_recv.at[half], to_right).wait_recv()

        @pl.when(half == 0)
        def _():
            copy_to(sent(0), sent(0), disp_send.at[0], disp_recv.at[0], to_right).wait_recv()

    def sent(half):
        rows = pl.ds(0, PART if half else PART - SLOTS)
        return rows_in.at[:, half // 2, rows, :] if IS_DIRECT[half] else rows_in.at[0, half // 2, rows, :]

    def to_next(half, block, device, side):
        r, at = half // 2, rows_of(half)
        return copy_to(
            rows_in.at[0, r, at, :], rows_in.at[block, r, at, :], ag_send, ag_recv.at[side, half], device
        )

    def gather_own(half):
        arrived(half)
        to_next(half, 1, to_right, 0).start()
        to_next(half, 2, to_left, 1).start()

    def gather_on(half):
        r, start = half // 2, half % 2 * PART
        for block, device, side in ((1, to_right, 0), (2, to_left, 1)):
            at = pl.ds(pl.multiple_of(start + side * QUARTER, QUARTER), QUARTER)
            to_next(half, block, device, side).wait_recv()
            copy_to(
                rows_in.at[block, r, at, :], rows_in.at[3, r, at, :], fwd_send, fwd_recv.at[half], device
            ).start()

    top, low = pl.ds(0, PART), pl.ds(PART, PART)

    def first_hop(r, side):
        at, device = ((top, to_right), (low, to_left))[side]
        return copy_to(parts.at[3, r, at, :], first_in.at[side * NZ + r], rs1_send, rs1_recv.at[side, r], device)

    def second_hop(r, side):
        device = (to_right, to_left)[side]
        return copy_to(second_out.at[side, r], second_in.at[side * NZ + r], rs2_send, rs2_recv.at[side, r], device)

    def experts(r):
        for part in range(2):
            half = 2 * r + part
            whole = rows_in.at[3, r, pl.ds(part * PART, PART), :]
            direct = is_direct(half)

            @pl.when(direct)
            def _():
                arrived(half)

            @pl.when(jnp.logical_not(direct))
            def _():
                copy_to(whole, whole, fwd_send, fwd_recv.at[half], to_right).wait_recv()

        gate_pre = jnp.zeros((ROWS, WIDTH), F32)
        up_pre = jnp.zeros((ROWS, WIDTH), F32)
        for k in range(NTP):
            block = rows_in[k, r]
            gate_pre = gate_pre + jnp.dot(block, wg[k], preferred_element_type=F32)
            up_pre = up_pre + jnp.dot(block, wu[k], preferred_element_type=F32)
        gate_held = jnp.minimum(gate_pre, LIMIT)
        up_held = jnp.clip(up_pre, -LIMIT, LIMIT)
        hidden = (gate_held * jax.nn.sigmoid(ALPHA * gate_held) * (up_held + 1.0)).astype(BF16)
        for k in (3, 1, 2, 0):
            parts[k, r] = jnp.dot(hidden, wd[k], preferred_element_type=F32).astype(BF16)
        first_hop(r, 0).start()
        first_hop(r, 1).start()

    def reduce_on(r):
        for side, (summing, plain) in enumerate(((top, low), (low, top))):
            first_hop(r, side).wait_recv()
            second_out[side, r, summing, :] = (
                parts[1 + side, r, summing, :].astype(F32) + first_in[side * NZ + r].astype(F32)
            ).astype(BF16)
            second_out[side, r, plain, :] = parts[1 + side, r, plain, :]
            second_hop(r, side).start()

    def send_back(r):
        second_hop(r, 0).wait_recv()
        second_hop(r, 1).wait_recv()
        reduced = parts[0, r].astype(F32) + second_in[r].astype(F32) + second_in[NZ + r].astype(F32)
        summed[r] = reduced.astype(BF16)
        source = (z - lookup(AWAY, r) + NZ) % NZ
        mine = pl.ds(pl.multiple_of(me * SLOTS, SLOTS), SLOTS)
        for i in range(8):
            there = source * PLANE + (x - i // 4 - 2 * (i % 4 // 2) + NX) % NX * 2 + i % 2
            at = pl.ds(i * SLOTS, SLOTS)

            @pl.when(there != me)
            def _():
                copy_to(
                    summed.at[r, at, :], ret.at[mine, :], ret_send, ret_recv.at[r], {"ep": there, "tp": y}
                ).start()

            if i < 2:

                @pl.when(there == me)
                def _():
                    ret[mine, :] = summed[r, at, :]

    def combine(r):
        for index in range(2):

            @pl.when((r == 0) == (index == 0))
            def _():
                every = ret.at[pl.ds(0, PLANE_ROWS - SLOTS if index == 0 else PLANE_ROWS), :]
                copy_to(every, every, ret_send, ret_recv.at[r], to_right).wait_recv()

        at = pl.ds(pl.multiple_of(ahead(r) * PLANE_ROWS, PLANE_ROWS), PLANE_ROWS)
        back = ret[at, :]
        for k in range(2):
            picked = jnp.dot(pick[k, :, at], back, preferred_element_type=F32)
            total[...] += picked * tk[k, :, NEP : NEP + 1]

    def picks(_):
        lane = lax.broadcasted_iota(I32, (NEP, NEP * SLOTS), 1)
        spread = (lane // SLOTS == lax.broadcasted_iota(I32, (NEP, NEP * SLOTS), 0)).astype(F32).astype(BF16)
        slot = (lax.broadcasted_iota(I32, (TOKENS, NEP * SLOTS), 1) % SLOTS).astype(F32)
        for k in range(2):
            ranks = jnp.dot(tk[k, :, 0:NEP].astype(BF16), spread, preferred_element_type=F32)
            pick[k] = (ranks == slot).astype(F32).astype(BF16)
        total[...] = jnp.zeros_like(total)

    def loaded(_):
        for load in loads[:12]:
            load.wait()

    def filtered(tile):
        @pl.when(tile == 0)
        def _():
            halo.wait()
            gbuf[0:32, :] = jnp.where(line == 0, 0.0, halo_in[...].astype(F32))

        conv(tile)

    def projected(chunk):
        @pl.when(chunk == 0)
        def _():
            loads[12].wait()

        project(chunk)

    actions = (
        dispatch, gather_own, gather_on, reduce_on, send_back, combine, experts, filtered, projected, picks, loaded,
    )

    def step(i, carry):
        place_in = i % 3
        shift = jnp.where(place_in == 0, jnp.int32(1), jnp.where(place_in == 1, jnp.int32(256), jnp.int32(65536)))
        code = lookup(WORDS, i // 3) // shift % 256
        kind, which = code // 16, code % 16
        for first, last in ((0, 3), (3, 7), (7, 11)):

            @pl.when(jnp.logical_and(kind >= first, kind < last))
            def _():
                for number in range(first, last):

                    @pl.when(kind == number)
                    def _():
                        actions[number](which)

        return carry

    lax.fori_loop(0, len(STEPS), step, 0)

    out_ref[...] = total[...].astype(BF16)

    for half in range(2 * NZ):
        copy_to(sent(half), sent(half), disp_send.at[half], disp_recv.at[half], to_right).wait_send()
    but_one = ret.at[pl.ds(0, (NEP - 1) * SLOTS), :]
    copy_to(but_one, but_one, ret_send, ret_recv.at[0], to_right).wait_send()
    some = second_in.at[pl.ds(0, GATHERED)]
    copy_to(some, some, ag_send, ret_recv.at[0], to_right).wait_send()
    copy_to(second_in, second_in, rs2_send, ret_recv.at[0], to_right).wait_send()
    some = first_in.at[pl.ds(0, GATHERED)]
    copy_to(some, some, fwd_send, ret_recv.at[0], to_right).wait_send()
    copy_to(first_in, first_in, rs1_send, ret_recv.at[0], to_right).wait_send()


def local(
    filter_value, filter_gate, filter_taps, filter_bias, norm_gain, norm_shift, out_weight, out_bias,
    expert_input, expert_gain, route_experts, route_weights, gate_weights, up_weights, down_weights,
):
    vmem = pl.BlockSpec(memory_space=pltpu.VMEM)
    hbm = pl.BlockSpec(memory_space=pltpu.HBM)
    dma = pltpu.SemaphoreType.DMA
    arguments = (
        filter_value, filter_gate, filter_taps, filter_bias[None], norm_gain[None], norm_shift[None],
        out_weight, out_bias[None], expert_input, expert_gain[None], route_experts.T, route_weights.T,
        gate_weights, up_weights, down_weights,
    )
    small = [argument for index, argument in enumerate(arguments[:12]) if index != 6]
    return pl.pallas_call(
        kernel,
        out_shape=(
            jax.ShapeDtypeStruct((TOKENS, 2048), BF16),
            jax.ShapeDtypeStruct((TOKENS, WIDTH), BF16),
        ),
        in_specs=[hbm] * len(arguments),
        out_specs=(vmem, vmem),
        scratch_shapes=[pltpu.VMEM(argument.shape, argument.dtype) for argument in small]
        + [
            pltpu.VMEM((NEP, TOKENS), BF16),
            pltpu.VMEM((2, TOKENS, 2 * NEP), F32),
            pltpu.VMEM((2, TOKENS, NEP * SLOTS), BF16),
            pltpu.VMEM((NTP, TOKENS, WIDTH), BF16),
            pltpu.VMEM((NTP, NZ, PLANE_ROWS, WIDTH), BF16),
            pltpu.VMEM((NTP, NZ, ROWS, WIDTH), BF16),
            pltpu.VMEM((NTP, WIDTH, WIDTH), BF16),
            pltpu.VMEM((NTP, WIDTH, WIDTH), BF16),
            pltpu.VMEM((NTP, WIDTH, WIDTH), BF16),
            pltpu.VMEM((CHANNELS, 2048), BF16),
            pltpu.VMEM((NTP, NZ, ROWS, WIDTH), BF16),
            pltpu.VMEM((2 * NZ, PART, WIDTH), BF16),
            pltpu.VMEM((2, NZ, ROWS, WIDTH), BF16),
            pltpu.VMEM((2 * NZ, ROWS, WIDTH), BF16),
            pltpu.VMEM((NZ, ROWS, WIDTH), BF16),
            pltpu.VMEM((NEP * SLOTS, WIDTH), BF16),
            pltpu.VMEM((TOKENS, WIDTH), F32),
            pltpu.VMEM((32, CHANNELS), BF16),
            pltpu.VMEM((32, CHANNELS), BF16),
            pltpu.VMEM((TOKENS + 32, CHANNELS), F32),
            pltpu.VMEM((TILE, CHANNELS), F32),
            pltpu.VMEM((TOKENS, CHANNELS), BF16),
            dma((11,)), dma((13,)),
            dma((2 * NZ,)), dma((2 * NZ,)), dma, dma((2, 2 * NZ)), dma, dma((2 * NZ,)),
            dma, dma((2, NZ)), dma, dma((2, NZ)), dma, dma((NZ,)), dma, dma,
        ],
        compiler_params=pltpu.CompilerParams(collective_id=0, has_side_effects=True, vmem_limit_bytes=46 * 1024 * 1024),
        name="filter_and_experts",
    )(*(pltpu.with_memory_space_constraint(argument, pltpu.HBM) for argument in arguments))


def solution(mesh):
    in_specs = (
        P(("ep", "tp"), None),
        P(("ep", "tp"), None),
        P(),
        P(),
        P(),
        P(),
        P(),
        P(),
        P("ep", None),
        P(),
        P("ep", None),
        P("ep", None),
        P("ep", None, "tp"),
        P("ep", None, "tp"),
        P("ep", "tp", None),
    )
    out_specs = (P(("ep", "tp"), None), P("ep", "tp"))
    return jax.shard_map(local, mesh=mesh, in_specs=in_specs, out_specs=out_specs, check_vma=False)
```

```python
import functools

import jax
import jax.numpy as jnp
from jax import lax
from jax.experimental import pallas as pl
from jax.experimental.pallas import tpu as pltpu
from jax.sharding import PartitionSpec as P

MESH = pl.DeviceIdType.MESH
BF16, F32, I32 = jnp.bfloat16, jnp.float32, jnp.int32

EPS = 1e-06
LIMIT = 7.0
ALPHA = 1.702

NZ = 8
NX = 4
PLANE = 8
NEP = 64
NTP = 4
SLOTS = 16
PLANE_ROWS = PLANE * SLOTS
TOKENS = 256
WIDTH = 512
AWAY = (0, 1, -1, 2, -2, 3, -3, 4)
DIRECT = (
    1, 2, 3, 4, 5, 6, 8,
)
SCHEDULE = (
    "S9 S11 S0 S1",
    "S12 S10 F3 S13",
    "S14 F2 S15 S7",
    "F1 A0 F0 S5",
    "S3 A9 P0 P1",
    "P2 B0 A11 P3",
    "G0 B9 A12 W0",
    "C0 B11 A10 S8",
    "S6 B12 A13 D0",
    "A7 B10 A14 S4",
    "S2 B13 A15 E0",
    "B7 C5 B14 C6",
    "B15 D5 R0 D6",
    "C7 E5 C4 C3",
    "E6 D7 D4 C2",
    "C1 D3 E7 E4",
    "D2 D1 R5 E3",
    "R6 E2 E1 R7",
    "R4 R3 R2 R1",
)
KINDS = "SABDERCFPGW"
STEPS = tuple(KINDS.index(word[0]) * 16 + int(word[1:]) for line in SCHEDULE for word in line.split())
WORDS = tuple(
    sum(step << 8 * at for at, step in enumerate(STEPS[first : first + 3])) for first in range(0, len(STEPS), 3)
)
ROWS = PLANE_ROWS
PART = ROWS // 2
QUARTER = PART // 2
IS_DIRECT = tuple(int(half in DIRECT) for half in range(2 * NZ))
GATHERED = 2 * NZ - len(DIRECT)
TAPS = 31
CHANNELS = 1024
TILE = 64


def copy_to(src, dst, send, recv, device):
    return pltpu.make_async_remote_copy(
        src_ref=src, dst_ref=dst, send_sem=send, recv_sem=recv, device_id=device, device_id_type=MESH
    )


def lookup(table, index):
    value = jnp.int32(table[0])
    for at, entry in enumerate(table):
        if at and entry != table[0]:
            value = jnp.where(index == at, jnp.int32(entry), value)
    return value


def is_direct(half):
    return lookup(IS_DIRECT, half) == 1


def kernel(
    value_hbm, gate_hbm, taps_hbm, fbias_hbm, ngain_hbm, nshift_hbm, ow_hbm, obias_hbm,
    xin_hbm, egain_hbm, routes_hbm, rweights_hbm, wg_hbm, wu_hbm, wd_hbm,
    mixer_ref, out_ref,
    value_ref, gate_ref, taps_ref, fbias_ref, ngain_ref, nshift_ref, obias_ref,
    xin_ref, egain_ref, routes_ref, rweights_ref,
    rm, tk, pick, nb, outgoing, rows_in, wg, wu, wd, ow, parts, first_in, second_out, second_in,
    summed, ret, total, halo_out, halo_in, gbuf, filt, act,
    early_sem, load_sem, disp_send, disp_recv, ag_send, ag_recv, fwd_send, fwd_recv,
    rs1_send, rs1_recv, rs2_send, rs2_recv, ret_send, ret_recv, halo_send, halo_recv,
):
    me = lax.axis_index("ep")
    y = lax.axis_index("tp")
    z, x, core = me // PLANE, me % PLANE // 2, me % 2
    right, left = (y + 1) % NTP, (y + NTP - 1) % NTP
    line = me * NTP + y
    after = (line + 1) % (NEP * NTP)
    to_right, to_left = {"ep": me, "tp": right}, {"ep": me, "tp": left}
    to_after = {"ep": after // NTP, "tp": after % NTP}

    early = [
        pltpu.make_async_copy(src, dst, early_sem.at[index])
        for index, (src, dst) in enumerate((
            (routes_hbm, routes_ref), (rweights_hbm, rweights_ref), (xin_hbm, xin_ref), (egain_hbm, egain_ref),
            (value_hbm, value_ref), (gate_hbm, gate_ref), (taps_hbm, taps_ref), (fbias_hbm, fbias_ref),
            (ngain_hbm, ngain_ref), (nshift_hbm, nshift_ref), (obias_hbm, obias_ref),
        ))
    ]
    for load in early[:4]:
        load.start()

    before = (line + NEP * NTP - 1) % (NEP * NTP)
    barrier = pltpu.get_barrier_semaphore()

    def greet(i, carry):
        peer = {"ep": (me + NEP // 2 + i) % NEP, "tp": y}
        pl.semaphore_signal(barrier, inc=1, device_id=peer, device_id_type=MESH)
        return carry

    lax.fori_loop(0, NEP // 2, greet, 0)
    lax.fori_loop(NEP // 2 + 1, NEP, greet, 0)
    for peer in (to_right, to_left, to_after, {"ep": before // NTP, "tp": before % NTP}):
        pl.semaphore_signal(barrier, inc=1, device_id=peer, device_id_type=MESH)

    for load in early[4:]:
        load.start()
    loads = []
    for k, shift in enumerate((0, 3, 1, 2)):
        at = pl.ds(pl.multiple_of((y + shift) % NTP * WIDTH, WIDTH), WIDTH)
        loads.append(pltpu.make_async_copy(wg_hbm.at[0, at, :], wg.at[k], load_sem.at[k]))
        loads.append(pltpu.make_async_copy(wu_hbm.at[0, at, :], wu.at[k], load_sem.at[4 + k]))
    for k, shift in enumerate((0, 1, 3, 2)):
        at = pl.ds(pl.multiple_of((y + shift) % NTP * WIDTH, WIDTH), WIDTH)
        loads.append(pltpu.make_async_copy(wd_hbm.at[0, :, at], wd.at[k], load_sem.at[8 + k]))
    loads.append(pltpu.make_async_copy(ow_hbm, ow, load_sem.at[12]))
    for load in loads:
        load.start()

    for load in early[:2]:
        load.wait()
    routes = routes_ref[...]
    expert = lax.broadcasted_iota(I32, (NEP, TOKENS), 0)
    named0 = routes[0:1, :] == expert
    named1 = routes[1:2, :] == expert
    named = jnp.logical_or(named0, named1)
    earlier = (
        lax.broadcasted_iota(I32, (TOKENS, TOKENS), 0) < lax.broadcasted_iota(I32, (TOKENS, TOKENS), 1)
    ).astype(F32).astype(BF16)
    rank = jnp.dot(named.astype(F32).astype(BF16), earlier, preferred_element_type=F32)
    rm[...] = jnp.where(named, rank, -1.0).astype(BF16)
    for k, hit in enumerate((named0, named1)):
        weight = jnp.broadcast_to(rweights_ref[k : k + 1, :], (NEP, TOKENS))
        tk[k] = jnp.concatenate([jnp.where(hit, rank, -1.0), weight], 0).T

    columns = [pl.ds(pl.multiple_of((y + shift) % NTP * WIDTH, WIDTH), WIDTH) for shift in (0, 3, 1, 2)]

    def normed(i, carry):
        at = pl.ds(pl.multiple_of(i * 16, 16), 16)
        tokens = xin_ref[at, :].astype(F32)
        scale = lax.rsqrt(jnp.mean(tokens * tokens, 1, keepdims=True) + EPS)
        for k in range(NTP):
            nb[k, at, :] = (xin_ref[at, columns[k]].astype(F32) * scale * egain_ref[0:1, columns[k]]).astype(BF16)
        return carry

    for load in early[2:4]:
        load.wait()
    lax.fori_loop(0, TOKENS // 16, normed, 0)

    row = lax.broadcasted_iota(I32, (PLANE_ROWS, NEP), 0)
    col = lax.broadcasted_iota(I32, (PLANE_ROWS, NEP), 1)
    slot_row = (lax.broadcasted_iota(I32, (PLANE_ROWS, TOKENS), 0) % SLOTS).astype(F32)

    def ahead(r):
        return (z + lookup(AWAY, r) + NZ) % NZ

    def place(r):
        spread = (row // SLOTS + ahead(r) * PLANE == col).astype(F32).astype(BF16)
        ranks = jnp.dot(spread, rm[...], preferred_element_type=F32)
        chosen = (ranks == slot_row).astype(F32).astype(BF16)
        for k in range(NTP if IS_DIRECT[2 * r] or IS_DIRECT[2 * r + 1] else 1):
            outgoing[k, r] = jnp.dot(chosen, nb[k], preferred_element_type=F32).astype(BF16)

    def dispatch(half):
        r, part = half // 2, half % 2
        direct = is_direct(half)
        for i in range(4):
            target = (x + part + 2 * (i // 2)) % NX * 2 + i % 2
            there = ahead(r) * PLANE + target
            at = pl.ds(pl.multiple_of(target * SLOTS, SLOTS), SLOTS)
            mine = pl.ds(pl.multiple_of(part * PART + (i // 2 * 2 + core) * SLOTS, SLOTS), SLOTS)

            @pl.when(jnp.logical_and(jnp.logical_not(direct), there != me))
            def _():
                copy_to(
                    outgoing.at[0, r, at, :], rows_in.at[0, r, mine, :],
                    disp_send.at[half], disp_recv.at[half], {"ep": there, "tp": y},
                ).start()

            @pl.when(jnp.logical_and(direct, there != me))
            def _():
                copy_to(
                    outgoing.at[:, r, at, :], rows_in.at[:, r, mine, :],
                    disp_send.at[half], disp_recv.at[half], {"ep": there, "tp": y},
                ).start()

            if i < 2:

                @pl.when(there == me)
                def _():
                    for k in range(NTP if IS_DIRECT[0] else 1):
                        rows_in[k, 0, mine, :] = outgoing[k, 0, at, :]

    def gated(i, carry):
        at = pl.ds(pl.multiple_of(i * 16, 16), 16)
        product = (value_ref[at, :].astype(F32) * jax.nn.sigmoid(gate_ref[at, :].astype(F32))).astype(BF16)
        gbuf[pl.ds(pl.multiple_of(i * 16 + 32, 16), 16), :] = product.astype(F32)

        @pl.when(i >= TOKENS // 16 - 2)
        def _():
            halo_out[pl.ds(pl.multiple_of(i * 16 - (TOKENS - 32), 16), 16), :] = product

        return carry

    for load in early[4:]:
        load.wait()
    lax.fori_loop(0, TOKENS // 16, gated, 0)
    for r in range(NZ):
        place(r)
    pl.semaphore_wait(barrier, NEP - 1 + 4)
    halo = copy_to(halo_out, halo_in, halo_send, halo_recv, to_after)
    halo.start()

    def conv(tile):
        def lanes(block, carry):
            at = pl.ds(pl.multiple_of(block * 128, 128), 128)
            window = gbuf[pl.ds(pl.multiple_of(tile * TILE, TILE), TILE + 32), at]
            value = jnp.broadcast_to(fbias_ref[0:1, at], (TILE, 128))
            for r in range(8):
                moved = window if r == 0 else pltpu.roll(window, TILE + 32 - r, 0)
                for q in range(5):
                    j = 8 * q + r - 2
                    if 0 <= j < TAPS:
                        value = value + taps_ref[j : j + 1, at] * moved[8 * q : 8 * q + TILE]
            filt[:, at] = value
            return carry

        lax.fori_loop(0, CHANNELS // 128, lanes, 0)

        def norm(i, carry):
            at = pl.ds(pl.multiple_of(i * 16, 16), 16)
            rows = filt[at, :]
            centred = rows - jnp.mean(rows, 1, keepdims=True)
            variance = jnp.mean(centred * centred, 1, keepdims=True)
            out = centred * lax.rsqrt(variance + EPS) * ngain_ref[0:1, :] + nshift_ref[0:1, :]
            act[pl.ds(pl.multiple_of(tile * TILE + i * 16, 16), 16), :] = (out * jax.nn.sigmoid(out)).astype(BF16)
            return carry

        lax.fori_loop(0, TILE // 16, norm, 0, unroll=True)

    def project(chunk):
        at = pl.ds(pl.multiple_of(chunk * 512, 512), 512)
        out = jnp.dot(act[...], ow[:, at], preferred_element_type=F32) + obias_ref[0:1, at]
        mixer_ref[:, at] = out.astype(BF16)

    def rows_of(half):
        return pl.ds(pl.multiple_of(half % 2 * PART, PART), PART)

    def arrived(half):
        r, direct, other = half // 2, is_direct(half), half != 0

        @pl.when(jnp.logical_and(jnp.logical_not(direct), other))
        def _():
            every = rows_in.at[0, r, rows_of(half), :]
            copy_to(every, every, disp_send.at[half], disp_recv.at[half], to_right).wait_recv()

        @pl.when(jnp.logical_and(direct, other))
        def _():
            every = rows_in.at[:, r, rows_of(half), :]
            copy_to(every, every, disp_send.at[half], disp_recv.at[half], to_right).wait_recv()

        @pl.when(half == 0)
        def _():
            copy_to(sent(0), sent(0), disp_send.at[0], disp_recv.at[0], to_right).wait_recv()

    def sent(half):
        rows = pl.ds(0, PART if half else PART - SLOTS)
        return rows_in.at[:, half // 2, rows, :] if IS_DIRECT[half] else rows_in.at[0, half // 2, rows, :]

    def to_next(half, block, device, side):
        r, at = half // 2, rows_of(half)
        return copy_to(
            rows_in.at[0, r, at, :], rows_in.at[block, r, at, :], ag_send, ag_recv.at[side, half], device
        )

    def gather_own(half):
        arrived(half)
        to_next(half, 1, to_right, 0).start()
        to_next(half, 2, to_left, 1).start()

    def gather_on(half):
        r, start = half // 2, half % 2 * PART
        for block, device, side in ((1, to_right, 0), (2, to_left, 1)):
            at = pl.ds(pl.multiple_of(start + side * QUARTER, QUARTER), QUARTER)
            to_next(half, block, device, side).wait_recv()
            copy_to(
                rows_in.at[block, r, at, :], rows_in.at[3, r, at, :], fwd_send, fwd_recv.at[half], device
            ).start()

    top, low = pl.ds(0, PART), pl.ds(PART, PART)

    def first_hop(r, side):
        at, device = ((top, to_right), (low, to_left))[side]
        return copy_to(parts.at[3, r, at, :], first_in.at[side * NZ + r], rs1_send, rs1_recv.at[side, r], device)

    def second_hop(r, side):
        device = (to_right, to_left)[side]
        return copy_to(second_out.at[side, r], second_in.at[side * NZ + r], rs2_send, rs2_recv.at[side, r], device)

    def experts(r):
        for part in range(2):
            half = 2 * r + part
            whole = rows_in.at[3, r, pl.ds(part * PART, PART), :]
            direct = is_direct(half)

            @pl.when(direct)
            def _():
                arrived(half)

            @pl.when(jnp.logical_not(direct))
            def _():
                copy_to(whole, whole, fwd_send, fwd_recv.at[half], to_right).wait_recv()

        gate_pre = jnp.zeros((ROWS, WIDTH), F32)
        up_pre = jnp.zeros((ROWS, WIDTH), F32)
        for k in range(NTP):
            block = rows_in[k, r]
            gate_pre = gate_pre + jnp.dot(block, wg[k], preferred_element_type=F32)
            up_pre = up_pre + jnp.dot(block, wu[k], preferred_element_type=F32)
        gate_held = jnp.minimum(gate_pre, LIMIT)
        up_held = jnp.clip(up_pre, -LIMIT, LIMIT)
        hidden = (gate_held * jax.nn.sigmoid(ALPHA * gate_held) * (up_held + 1.0)).astype(BF16)
        for k in (3, 1, 2, 0):
            parts[k, r] = jnp.dot(hidden, wd[k], preferred_element_type=F32).astype(BF16)
        first_hop(r, 0).start()
        first_hop(r, 1).start()

    def reduce_on(r):
        for side, (summing, plain) in enumerate(((top, low), (low, top))):
            first_hop(r, side).wait_recv()
            second_out[side, r, summing, :] = (
                parts[1 + side, r, summing, :].astype(F32) + first_in[side * NZ + r].astype(F32)
            ).astype(BF16)
            second_out[side, r, plain, :] = parts[1 + side, r, plain, :]
            second_hop(r, side).start()

    def send_back(r):
        second_hop(r, 0).wait_recv()
        second_hop(r, 1).wait_recv()
        reduced = parts[0, r].astype(F32) + second_in[r].astype(F32) + second_in[NZ + r].astype(F32)
        summed[r] = reduced.astype(BF16)
        source = (z - lookup(AWAY, r) + NZ) % NZ
        mine = pl.ds(pl.multiple_of(me * SLOTS, SLOTS), SLOTS)
        for i in range(8):
            there = source * PLANE + (x - i // 4 - 2 * (i % 4 // 2) + NX) % NX * 2 + i % 2
            at = pl.ds(i * SLOTS, SLOTS)

            @pl.when(there != me)
            def _():
                copy_to(
                    summed.at[r, at, :], ret.at[mine, :], ret_send, ret_recv.at[r], {"ep": there, "tp": y}
                ).start()

            if i < 2:

                @pl.when(there == me)
                def _():
                    ret[mine, :] = summed[r, at, :]

    def combine(r):
        for index in range(2):

            @pl.when((r == 0) == (index == 0))
            def _():
                every = ret.at[pl.ds(0, PLANE_ROWS - SLOTS if index == 0 else PLANE_ROWS), :]
                copy_to(every, every, ret_send, ret_recv.at[r], to_right).wait_recv()

        at = pl.ds(pl.multiple_of(ahead(r) * PLANE_ROWS, PLANE_ROWS), PLANE_ROWS)
        back = ret[at, :]
        for k in range(2):
            picked = jnp.dot(pick[k, :, at], back, preferred_element_type=F32)
            total[...] += picked * tk[k, :, NEP : NEP + 1]

    def picks(_):
        lane = lax.broadcasted_iota(I32, (NEP, NEP * SLOTS), 1)
        spread = (lane // SLOTS == lax.broadcasted_iota(I32, (NEP, NEP * SLOTS), 0)).astype(F32).astype(BF16)
        slot = (lax.broadcasted_iota(I32, (TOKENS, NEP * SLOTS), 1) % SLOTS).astype(F32)
        for k in range(2):
            ranks = jnp.dot(tk[k, :, 0:NEP].astype(BF16), spread, preferred_element_type=F32)
            pick[k] = (ranks == slot).astype(F32).astype(BF16)
        total[...] = jnp.zeros_like(total)

    def loaded(_):
        for load in loads[:12]:
            load.wait()

    def filtered(tile):
        @pl.when(tile == 0)
        def _():
            halo.wait()
            gbuf[0:32, :] = jnp.where(line == 0, 0.0, halo_in[...].astype(F32))

        conv(tile)

    def projected(chunk):
        @pl.when(chunk == 0)
        def _():
            loads[12].wait()

        project(chunk)

    actions = (
        dispatch, gather_own, gather_on, reduce_on, send_back, combine, experts, filtered, projected, picks, loaded,
    )

    def step(i, carry):
        place_in = i % 3
        shift = jnp.where(place_in == 0, jnp.int32(1), jnp.where(place_in == 1, jnp.int32(256), jnp.int32(65536)))
        code = lookup(WORDS, i // 3) // shift % 256
        kind, which = code // 16, code % 16
        for first, last in ((0, 3), (3, 7), (7, 11)):

            @pl.when(jnp.logical_and(kind >= first, kind < last))
            def _():
                for number in range(first, last):

                    @pl.when(kind == number)
                    def _():
                        actions[number](which)

        return carry

    lax.fori_loop(0, len(STEPS), step, 0)

    out_ref[...] = total[...].astype(BF16)

    for half in range(2 * NZ):
        copy_to(sent(half), sent(half), disp_send.at[half], disp_recv.at[half], to_right).wait_send()
    but_one = ret.at[pl.ds(0, (NEP - 1) * SLOTS), :]
    copy_to(but_one, but_one, ret_send, ret_recv.at[0], to_right).wait_send()
    some = second_in.at[pl.ds(0, GATHERED)]
    copy_to(some, some, ag_send, ret_recv.at[0], to_right).wait_send()
    copy_to(second_in, second_in, rs2_send, ret_recv.at[0], to_right).wait_send()
    some = first_in.at[pl.ds(0, GATHERED)]
    copy_to(some, some, fwd_send, ret_recv.at[0], to_right).wait_send()
    copy_to(first_in, first_in, rs1_send, ret_recv.at[0], to_right).wait_send()


def hand_over(mixer_ref, out_ref, mixer_hbm, out_hbm, sem):
    copies = [
        pltpu.make_async_copy(mixer_ref, mixer_hbm, sem.at[0]),
        pltpu.make_async_copy(out_ref, out_hbm, sem.at[1]),
    ]
    for copy in copies:
        copy.start()
    for copy in copies:
        copy.wait()


def local(
    filter_value, filter_gate, filter_taps, filter_bias, norm_gain, norm_shift, out_weight, out_bias,
    expert_input, expert_gain, route_experts, route_weights, gate_weights, up_weights, down_weights,
):
    vmem = pl.BlockSpec(memory_space=pltpu.VMEM)
    hbm = pl.BlockSpec(memory_space=pltpu.HBM)
    dma = pltpu.SemaphoreType.DMA
    arguments = (
        filter_value, filter_gate, filter_taps, filter_bias[None], norm_gain[None], norm_shift[None],
        out_weight, out_bias[None], expert_input, expert_gain[None], route_experts.T, route_weights.T,
        gate_weights, up_weights, down_weights,
    )
    small = [argument for index, argument in enumerate(arguments[:12]) if index != 6]
    shapes = (jax.ShapeDtypeStruct((TOKENS, 2048), BF16), jax.ShapeDtypeStruct((TOKENS, WIDTH), BF16))
    results = pl.pallas_call(
        kernel,
        out_shape=shapes,
        in_specs=[hbm] * len(arguments),
        out_specs=(vmem, vmem),
        scratch_shapes=[pltpu.VMEM(argument.shape, argument.dtype) for argument in small]
        + [
            pltpu.VMEM((NEP, TOKENS), BF16),
            pltpu.VMEM((2, TOKENS, 2 * NEP), F32),
            pltpu.VMEM((2, TOKENS, NEP * SLOTS), BF16),
            pltpu.VMEM((NTP, TOKENS, WIDTH), BF16),
            pltpu.VMEM((NTP, NZ, PLANE_ROWS, WIDTH), BF16),
            pltpu.VMEM((NTP, NZ, ROWS, WIDTH), BF16),
            pltpu.VMEM((NTP, WIDTH, WIDTH), BF16),
            pltpu.VMEM((NTP, WIDTH, WIDTH), BF16),
            pltpu.VMEM((NTP, WIDTH, WIDTH), BF16),
            pltpu.VMEM((CHANNELS, 2048), BF16),
            pltpu.VMEM((NTP, NZ, ROWS, WIDTH), BF16),
            pltpu.VMEM((2 * NZ, PART, WIDTH), BF16),
            pltpu.VMEM((2, NZ, ROWS, WIDTH), BF16),
            pltpu.VMEM((2 * NZ, ROWS, WIDTH), BF16),
            pltpu.VMEM((NZ, ROWS, WIDTH), BF16),
            pltpu.VMEM((NEP * SLOTS, WIDTH), BF16),
            pltpu.VMEM((TOKENS, WIDTH), F32),
            pltpu.VMEM((32, CHANNELS), BF16),
            pltpu.VMEM((32, CHANNELS), BF16),
            pltpu.VMEM((TOKENS + 32, CHANNELS), F32),
            pltpu.VMEM((TILE, CHANNELS), F32),
            pltpu.VMEM((TOKENS, CHANNELS), BF16),
            dma((11,)), dma((13,)),
            dma((2 * NZ,)), dma((2 * NZ,)), dma, dma((2, 2 * NZ)), dma, dma((2 * NZ,)),
            dma, dma((2, NZ)), dma, dma((2, NZ)), dma, dma((NZ,)), dma, dma,
        ],
        compiler_params=pltpu.CompilerParams(collective_id=0, has_side_effects=True, vmem_limit_bytes=46 * 1024 * 1024),
        name="filter_and_experts",
    )(*(pltpu.with_memory_space_constraint(argument, pltpu.HBM) for argument in arguments))
    return pl.pallas_call(
        hand_over,
        out_shape=shapes,
        in_specs=[vmem] * 2,
        out_specs=(hbm, hbm),
        scratch_shapes=[dma((2,))],
        compiler_params=pltpu.CompilerParams(vmem_limit_bytes=4 * 1024 * 1024),
        name="hand_over",
    )(*(pltpu.with_memory_space_constraint(result, pltpu.VMEM) for result in results))


def solution(mesh):
    in_specs = (
        P(("ep", "tp"), None),
        P(("ep", "tp"), None),
        P(),
        P(),
        P(),
        P(),
        P(),
        P(),
        P("ep", None),
        P(),
        P("ep", None),
        P("ep", None),
        P("ep", None, "tp"),
        P("ep", None, "tp"),
        P("ep", "tp", None),
    )
    out_specs = (P(("ep", "tp"), None), P("ep", "tp"))
    return jax.shard_map(local, mesh=mesh, in_specs=in_specs, out_specs=out_specs, check_vma=False)
```

```python
import functools

import jax
import jax.numpy as jnp
from jax import lax
from jax.experimental import pallas as pl
from jax.experimental.pallas import tpu as pltpu
from jax.sharding import PartitionSpec as P

MESH = pl.DeviceIdType.MESH
BF16, F32, I32 = jnp.bfloat16, jnp.float32, jnp.int32

EPS = 1e-06
LIMIT = 7.0
ALPHA = 1.702

NZ = 8
NX = 4
PLANE = 8
NEP = 64
NTP = 4
SLOTS = 16
PLANE_ROWS = PLANE * SLOTS
TOKENS = 256
WIDTH = 512
AWAY = (0, 1, -1, 2, -2, 3, -3, 4)
DIRECT = (
    1, 2, 3, 4, 5, 6, 8,
)
SCHEDULE = (
    "S9 S11 S0 S1",
    "S12 S10 F3 S13",
    "S14 F2 S15 S7",
    "F1 A0 F0 S5",
    "S3 A9 P0 P1",
    "P2 B0 A11 P3",
    "G0 B9 A12 W0",
    "C0 B11 A10 S8",
    "S6 B12 A13 D0",
    "A7 B10 A14 S4",
    "S2 B13 A15 E0",
    "B7 C5 B14 C6",
    "B15 D5 R0 D6",
    "C7 E5 C4 C3",
    "E6 D7 D4 C2",
    "C1 D3 E7 E4",
    "D2 D1 R5 E3",
    "R6 E2 E1 R7",
    "R4 R3 R2 R1",
)
KINDS = "SABDERCFPGW"
STEPS = tuple(KINDS.index(word[0]) * 16 + int(word[1:]) for line in SCHEDULE for word in line.split())
WORDS = tuple(
    sum(step << 8 * at for at, step in enumerate(STEPS[first : first + 3])) for first in range(0, len(STEPS), 3)
)
ROWS = PLANE_ROWS
PART = ROWS // 2
QUARTER = PART // 2
IS_DIRECT = tuple(int(half in DIRECT) for half in range(2 * NZ))
GATHERED = 2 * NZ - len(DIRECT)
TAPS = 31
CHANNELS = 1024
TILE = 64


def copy_to(src, dst, send, recv, device):
    return pltpu.make_async_remote_copy(
        src_ref=src, dst_ref=dst, send_sem=send, recv_sem=recv, device_id=device, device_id_type=MESH
    )


def lookup(table, index):
    value = jnp.int32(table[0])
    for at, entry in enumerate(table):
        if at and entry != table[0]:
            value = jnp.where(index == at, jnp.int32(entry), value)
    return value


def is_direct(half):
    return lookup(IS_DIRECT, half) == 1


def kernel(
    value_hbm, gate_hbm, taps_hbm, fbias_hbm, ngain_hbm, nshift_hbm, ow_hbm, obias_hbm,
    xin_hbm, egain_hbm, routes_hbm, rweights_hbm, wg_hbm, wu_hbm, wd_hbm,
    mixer_ref, out_ref,
    value_ref, gate_ref, taps_ref, fbias_ref, ngain_ref, nshift_ref, obias_ref,
    xin_ref, egain_ref, routes_ref, rweights_ref,
    rm, tk, pick, nb, outgoing, rows_in, wg, wu, wd, ow, parts, first_in, second_out, second_in,
    summed, ret, total, halo_out, halo_in, gbuf, filt, act,
    early_sem, load_sem, disp_send, disp_recv, ag_send, ag_recv, fwd_send, fwd_recv,
    rs1_send, rs1_recv, rs2_send, rs2_recv, ret_send, ret_recv, halo_send, halo_recv,
):
    me = lax.axis_index("ep")
    y = lax.axis_index("tp")
    z, x, core = me // PLANE, me % PLANE // 2, me % 2
    right, left = (y + 1) % NTP, (y + NTP - 1) % NTP
    line = me * NTP + y
    after = (line + 1) % (NEP * NTP)
    to_right, to_left = {"ep": me, "tp": right}, {"ep": me, "tp": left}
    to_after = {"ep": after // NTP, "tp": after % NTP}

    early = [
        pltpu.make_async_copy(src, dst, early_sem.at[index])
        for index, (src, dst) in enumerate((
            (routes_hbm, routes_ref), (rweights_hbm, rweights_ref), (xin_hbm, xin_ref), (egain_hbm, egain_ref),
            (value_hbm, value_ref), (gate_hbm, gate_ref), (taps_hbm, taps_ref), (fbias_hbm, fbias_ref),
            (ngain_hbm, ngain_ref), (nshift_hbm, nshift_ref), (obias_hbm, obias_ref),
        ))
    ]
    for load in early[:4]:
        load.start()

    before = (line + NEP * NTP - 1) % (NEP * NTP)
    barrier = pltpu.get_barrier_semaphore()

    def greet(i, carry):
        peer = {"ep": (me + NEP // 2 + i) % NEP, "tp": y}
        pl.semaphore_signal(barrier, inc=1, device_id=peer, device_id_type=MESH)
        return carry

    lax.fori_loop(0, NEP // 2, greet, 0, unroll=True)
    lax.fori_loop(NEP // 2 + 1, NEP, greet, 0, unroll=True)
    for peer in (to_right, to_left, to_after, {"ep": before // NTP, "tp": before % NTP}):
        pl.semaphore_signal(barrier, inc=1, device_id=peer, device_id_type=MESH)

    for load in early[4:]:
        load.start()
    loads = []
    for k, shift in enumerate((0, 3, 1, 2)):
        at = pl.ds(pl.multiple_of((y + shift) % NTP * WIDTH, WIDTH), WIDTH)
        loads.append(pltpu.make_async_copy(wg_hbm.at[0, at, :], wg.at[k], load_sem.at[k]))
        loads.append(pltpu.make_async_copy(wu_hbm.at[0, at, :], wu.at[k], load_sem.at[4 + k]))
    for k, shift in enumerate((0, 1, 3, 2)):
        at = pl.ds(pl.multiple_of((y + shift) % NTP * WIDTH, WIDTH), WIDTH)
        loads.append(pltpu.make_async_copy(wd_hbm.at[0, :, at], wd.at[k], load_sem.at[8 + k]))
    loads.append(pltpu.make_async_copy(ow_hbm, ow, load_sem.at[12]))
    for load in loads:
        load.start()

    for load in early[:2]:
        load.wait()
    routes = routes_ref[...]
    expert = lax.broadcasted_iota(I32, (NEP, TOKENS), 0)
    named0 = routes[0:1, :] == expert
    named1 = routes[1:2, :] == expert
    named = jnp.logical_or(named0, named1)
    earlier = (
        lax.broadcasted_iota(I32, (TOKENS, TOKENS), 0) < lax.broadcasted_iota(I32, (TOKENS, TOKENS), 1)
    ).astype(F32).astype(BF16)
    rank = jnp.dot(named.astype(F32).astype(BF16), earlier, preferred_element_type=F32)
    rm[...] = jnp.where(named, rank, -1.0).astype(BF16)
    for k, hit in enumerate((named0, named1)):
        weight = jnp.broadcast_to(rweights_ref[k : k + 1, :], (NEP, TOKENS))
        tk[k] = jnp.concatenate([jnp.where(hit, rank, -1.0), weight], 0).T

    columns = [pl.ds(pl.multiple_of((y + shift) % NTP * WIDTH, WIDTH), WIDTH) for shift in (0, 3, 1, 2)]

    def normed(i, carry):
        at = pl.ds(pl.multiple_of(i * 16, 16), 16)
        tokens = xin_ref[at, :].astype(F32)
        scale = lax.rsqrt(jnp.mean(tokens * tokens, 1, keepdims=True) + EPS)
        for k in range(NTP):
            nb[k, at, :] = (xin_ref[at, columns[k]].astype(F32) * scale * egain_ref[0:1, columns[k]]).astype(BF16)
        return carry

    for load in early[2:4]:
        load.wait()
    lax.fori_loop(0, TOKENS // 16, normed, 0)

    row = lax.broadcasted_iota(I32, (PLANE_ROWS, NEP), 0)
    col = lax.broadcasted_iota(I32, (PLANE_ROWS, NEP), 1)
    slot_row = (lax.broadcasted_iota(I32, (PLANE_ROWS, TOKENS), 0) % SLOTS).astype(F32)

    def ahead(r):
        return (z + lookup(AWAY, r) + NZ) % NZ

    def place(r):
        spread = (row // SLOTS + ahead(r) * PLANE == col).astype(F32).astype(BF16)
        ranks = jnp.dot(spread, rm[...], preferred_element_type=F32)
        chosen = (ranks == slot_row).astype(F32).astype(BF16)
        for k in range(NTP if IS_DIRECT[2 * r] or IS_DIRECT[2 * r + 1] else 1):
            outgoing[k, r] = jnp.dot(chosen, nb[k], preferred_element_type=F32).astype(BF16)

    def dispatch(half):
        r, part = half // 2, half % 2
        direct = is_direct(half)
        for i in range(4):
            target = (x + part + 2 * (i // 2)) % NX * 2 + i % 2
            there = ahead(r) * PLANE + target
            at = pl.ds(pl.multiple_of(target * SLOTS, SLOTS), SLOTS)
            mine = pl.ds(pl.multiple_of(part * PART + (i // 2 * 2 + core) * SLOTS, SLOTS), SLOTS)

            @pl.when(jnp.logical_and(jnp.logical_not(direct), there != me))
            def _():
                copy_to(
                    outgoing.at[0, r, at, :], rows_in.at[0, r, mine, :],
                    disp_send.at[half], disp_recv.at[half], {"ep": there, "tp": y},
                ).start()

            @pl.when(jnp.logical_and(direct, there != me))
            def _():
                copy_to(
                    outgoing.at[:, r, at, :], rows_in.at[:, r, mine, :],
                    disp_send.at[half], disp_recv.at[half], {"ep": there, "tp": y},
                ).start()

            if i < 2:

                @pl.when(there == me)
                def _():
                    for k in range(NTP if IS_DIRECT[0] else 1):
                        rows_in[k, 0, mine, :] = outgoing[k, 0, at, :]

    def gated(i, carry):
        at = pl.ds(pl.multiple_of(i * 16, 16), 16)
        product = (value_ref[at, :].astype(F32) * jax.nn.sigmoid(gate_ref[at, :].astype(F32))).astype(BF16)
        gbuf[pl.ds(pl.multiple_of(i * 16 + 32, 16), 16), :] = product.astype(F32)

        @pl.when(i >= TOKENS // 16 - 2)
        def _():
            halo_out[pl.ds(pl.multiple_of(i * 16 - (TOKENS - 32), 16), 16), :] = product

        return carry

    for load in early[4:]:
        load.wait()
    lax.fori_loop(0, TOKENS // 16, gated, 0)
    for r in range(NZ):
        place(r)
    pl.semaphore_wait(barrier, NEP - 1 + 4)
    halo = copy_to(halo_out, halo_in, halo_send, halo_recv, to_after)
    halo.start()

    def conv(tile):
        def lanes(block, carry):
            at = pl.ds(pl.multiple_of(block * 128, 128), 128)
            window = gbuf[pl.ds(pl.multiple_of(tile * TILE, TILE), TILE + 32), at]
            value = jnp.broadcast_to(fbias_ref[0:1, at], (TILE, 128))
            for r in range(8):
                moved = window if r == 0 else pltpu.roll(window, TILE + 32 - r, 0)
                for q in range(5):
                    j = 8 * q + r - 2
                    if 0 <= j < TAPS:
                        value = value + taps_ref[j : j + 1, at] * moved[8 * q : 8 * q + TILE]
            filt[:, at] = value
            return carry

        lax.fori_loop(0, CHANNELS // 128, lanes, 0)

        def norm(i, carry):
            at = pl.ds(pl.multiple_of(i * 16, 16), 16)
            rows = filt[at, :]
            centred = rows - jnp.mean(rows, 1, keepdims=True)
            variance = jnp.mean(centred * centred, 1, keepdims=True)
            out = centred * lax.rsqrt(variance + EPS) * ngain_ref[0:1, :] + nshift_ref[0:1, :]
            act[pl.ds(pl.multiple_of(tile * TILE + i * 16, 16), 16), :] = (out * jax.nn.sigmoid(out)).astype(BF16)
            return carry

        lax.fori_loop(0, TILE // 16, norm, 0, unroll=True)

    def project(chunk):
        at = pl.ds(pl.multiple_of(chunk * 512, 512), 512)
        out = jnp.dot(act[...], ow[:, at], preferred_element_type=F32) + obias_ref[0:1, at]
        mixer_ref[:, at] = out.astype(BF16)

    def rows_of(half):
        return pl.ds(pl.multiple_of(half % 2 * PART, PART), PART)

    def arrived(half):
        r, direct, other = half // 2, is_direct(half), half != 0

        @pl.when(jnp.logical_and(jnp.logical_not(direct), other))
        def _():
            every = rows_in.at[0, r, rows_of(half), :]
            copy_to(every, every, disp_send.at[half], disp_recv.at[half], to_right).wait_recv()

        @pl.when(jnp.logical_and(direct, other))
        def _():
            every = rows_in.at[:, r, rows_of(half), :]
            copy_to(every, every, disp_send.at[half], disp_recv.at[half], to_right).wait_recv()

        @pl.when(half == 0)
        def _():
            copy_to(sent(0), sent(0), disp_send.at[0], disp_recv.at[0], to_right).wait_recv()

    def sent(half):
        rows = pl.ds(0, PART if half else PART - SLOTS)
        return rows_in.at[:, half // 2, rows, :] if IS_DIRECT[half] else rows_in.at[0, half // 2, rows, :]

    def to_next(half, block, device, side):
        r, at = half // 2, rows_of(half)
        return copy_to(
            rows_in.at[0, r, at, :], rows_in.at[block, r, at, :], ag_send, ag_recv.at[side, half], device
        )

    def gather_own(half):
        arrived(half)
        to_next(half, 1, to_right, 0).start()
        to_next(half, 2, to_left, 1).start()

    def gather_on(half):
        r, start = half // 2, half % 2 * PART
        for block, device, side in ((1, to_right, 0), (2, to_left, 1)):
            at = pl.ds(pl.multiple_of(start + side * QUARTER, QUARTER), QUARTER)
            to_next(half, block, device, side).wait_recv()
            copy_to(
                rows_in.at[block, r, at, :], rows_in.at[3, r, at, :], fwd_send, fwd_recv.at[half], device
            ).start()

    top, low = pl.ds(0, PART), pl.ds(PART, PART)

    def first_hop(r, side):
        at, device = ((top, to_right), (low, to_left))[side]
        return copy_to(parts.at[3, r, at, :], first_in.at[side * NZ + r], rs1_send, rs1_recv.at[side, r], device)

    def second_hop(r, side):
        device = (to_right, to_left)[side]
        return copy_to(second_out.at[side, r], second_in.at[side * NZ + r], rs2_send, rs2_recv.at[side, r], device)

    def experts(r):
        for part in range(2):
            half = 2 * r + part
            whole = rows_in.at[3, r, pl.ds(part * PART, PART), :]
            direct = is_direct(half)

            @pl.when(direct)
            def _():
                arrived(half)

            @pl.when(jnp.logical_not(direct))
            def _():
                copy_to(whole, whole, fwd_send, fwd_recv.at[half], to_right).wait_recv()

        gate_pre = jnp.zeros((ROWS, WIDTH), F32)
        up_pre = jnp.zeros((ROWS, WIDTH), F32)
        for k in range(NTP):
            block = rows_in[k, r]
            gate_pre = gate_pre + jnp.dot(block, wg[k], preferred_element_type=F32)
            up_pre = up_pre + jnp.dot(block, wu[k], preferred_element_type=F32)
        gate_held = jnp.minimum(gate_pre, LIMIT)
        up_held = jnp.clip(up_pre, -LIMIT, LIMIT)
        hidden = (gate_held * jax.nn.sigmoid(ALPHA * gate_held) * (up_held + 1.0)).astype(BF16)
        for k in (3, 1, 2, 0):
            parts[k, r] = jnp.dot(hidden, wd[k], preferred_element_type=F32).astype(BF16)
        first_hop(r, 0).start()
        first_hop(r, 1).start()

    def reduce_on(r):
        for side, (summing, plain) in enumerate(((top, low), (low, top))):
            first_hop(r, side).wait_recv()
            second_out[side, r, summing, :] = (
                parts[1 + side, r, summing, :].astype(F32) + first_in[side * NZ + r].astype(F32)
            ).astype(BF16)
            second_out[side, r, plain, :] = parts[1 + side, r, plain, :]
            second_hop(r, side).start()

    def send_back(r):
        second_hop(r, 0).wait_recv()
        second_hop(r, 1).wait_recv()
        reduced = parts[0, r].astype(F32) + second_in[r].astype(F32) + second_in[NZ + r].astype(F32)
        summed[r] = reduced.astype(BF16)
        source = (z - lookup(AWAY, r) + NZ) % NZ
        mine = pl.ds(pl.multiple_of(me * SLOTS, SLOTS), SLOTS)
        for i in range(8):
            there = source * PLANE + (x - i // 4 - 2 * (i % 4 // 2) + NX) % NX * 2 + i % 2
            at = pl.ds(i * SLOTS, SLOTS)

            @pl.when(there != me)
            def _():
                copy_to(
                    summed.at[r, at, :], ret.at[mine, :], ret_send, ret_recv.at[r], {"ep": there, "tp": y}
                ).start()

            if i < 2:

                @pl.when(there == me)
                def _():
                    ret[mine, :] = summed[r, at, :]

    def combine(r):
        for index in range(2):

            @pl.when((r == 0) == (index == 0))
            def _():
                every = ret.at[pl.ds(0, PLANE_ROWS - SLOTS if index == 0 else PLANE_ROWS), :]
                copy_to(every, every, ret_send, ret_recv.at[r], to_right).wait_recv()

        at = pl.ds(pl.multiple_of(ahead(r) * PLANE_ROWS, PLANE_ROWS), PLANE_ROWS)
        back = ret[at, :]
        for k in range(2):
            picked = jnp.dot(pick[k, :, at], back, preferred_element_type=F32)
            total[...] += picked * tk[k, :, NEP : NEP + 1]

    def picks(_):
        lane = lax.broadcasted_iota(I32, (NEP, NEP * SLOTS), 1)
        spread = (lane // SLOTS == lax.broadcasted_iota(I32, (NEP, NEP * SLOTS), 0)).astype(F32).astype(BF16)
        slot = (lax.broadcasted_iota(I32, (TOKENS, NEP * SLOTS), 1) % SLOTS).astype(F32)
        for k in range(2):
            ranks = jnp.dot(tk[k, :, 0:NEP].astype(BF16), spread, preferred_element_type=F32)
            pick[k] = (ranks == slot).astype(F32).astype(BF16)
        total[...] = jnp.zeros_like(total)

    def loaded(_):
        for load in loads[:12]:
            load.wait()

    def filtered(tile):
        @pl.when(tile == 0)
        def _():
            halo.wait()
            gbuf[0:32, :] = jnp.where(line == 0, 0.0, halo_in[...].astype(F32))

        conv(tile)

    def projected(chunk):
        @pl.when(chunk == 0)
        def _():
            loads[12].wait()

        project(chunk)

    actions = (
        dispatch, gather_own, gather_on, reduce_on, send_back, combine, experts, filtered, projected, picks, loaded,
    )

    def step(i, carry):
        place_in = i % 3
        shift = jnp.where(place_in == 0, jnp.int32(1), jnp.where(place_in == 1, jnp.int32(256), jnp.int32(65536)))
        code = lookup(WORDS, i // 3) // shift % 256
        kind, which = code // 16, code % 16
        for first, last in ((0, 3), (3, 7), (7, 11)):

            @pl.when(jnp.logical_and(kind >= first, kind < last))
            def _():
                for number in range(first, last):

                    @pl.when(kind == number)
                    def _():
                        actions[number](which)

        return carry

    lax.fori_loop(0, len(STEPS), step, 0)

    out_ref[...] = total[...].astype(BF16)

    for half in range(2 * NZ):
        copy_to(sent(half), sent(half), disp_send.at[half], disp_recv.at[half], to_right).wait_send()
    but_one = ret.at[pl.ds(0, (NEP - 1) * SLOTS), :]
    copy_to(but_one, but_one, ret_send, ret_recv.at[0], to_right).wait_send()
    some = second_in.at[pl.ds(0, GATHERED)]
    copy_to(some, some, ag_send, ret_recv.at[0], to_right).wait_send()
    copy_to(second_in, second_in, rs2_send, ret_recv.at[0], to_right).wait_send()
    some = first_in.at[pl.ds(0, GATHERED)]
    copy_to(some, some, fwd_send, ret_recv.at[0], to_right).wait_send()
    copy_to(first_in, first_in, rs1_send, ret_recv.at[0], to_right).wait_send()


def hand_over(mixer_ref, out_ref, mixer_hbm, out_hbm, sem):
    copies = [
        pltpu.make_async_copy(mixer_ref, mixer_hbm, sem.at[0]),
        pltpu.make_async_copy(out_ref, out_hbm, sem.at[1]),
    ]
    for copy in copies:
        copy.start()
    for copy in copies:
        copy.wait()


def local(
    filter_value, filter_gate, filter_taps, filter_bias, norm_gain, norm_shift, out_weight, out_bias,
    expert_input, expert_gain, route_experts, route_weights, gate_weights, up_weights, down_weights,
):
    vmem = pl.BlockSpec(memory_space=pltpu.VMEM)
    hbm = pl.BlockSpec(memory_space=pltpu.HBM)
    dma = pltpu.SemaphoreType.DMA
    arguments = (
        filter_value, filter_gate, filter_taps, filter_bias[None], norm_gain[None], norm_shift[None],
        out_weight, out_bias[None], expert_input, expert_gain[None], route_experts.T, route_weights.T,
        gate_weights, up_weights, down_weights,
    )
    small = [argument for index, argument in enumerate(arguments[:12]) if index != 6]
    shapes = (jax.ShapeDtypeStruct((TOKENS, 2048), BF16), jax.ShapeDtypeStruct((TOKENS, WIDTH), BF16))
    results = pl.pallas_call(
        kernel,
        out_shape=shapes,
        in_specs=[hbm] * len(arguments),
        out_specs=(vmem, vmem),
        scratch_shapes=[pltpu.VMEM(argument.shape, argument.dtype) for argument in small]
        + [
            pltpu.VMEM((NEP, TOKENS), BF16),
            pltpu.VMEM((2, TOKENS, 2 * NEP), F32),
            pltpu.VMEM((2, TOKENS, NEP * SLOTS), BF16),
            pltpu.VMEM((NTP, TOKENS, WIDTH), BF16),
            pltpu.VMEM((NTP, NZ, PLANE_ROWS, WIDTH), BF16),
            pltpu.VMEM((NTP, NZ, ROWS, WIDTH), BF16),
            pltpu.VMEM((NTP, WIDTH, WIDTH), BF16),
            pltpu.VMEM((NTP, WIDTH, WIDTH), BF16),
            pltpu.VMEM((NTP, WIDTH, WIDTH), BF16),
            pltpu.VMEM((CHANNELS, 2048), BF16),
            pltpu.VMEM((NTP, NZ, ROWS, WIDTH), BF16),
            pltpu.VMEM((2 * NZ, PART, WIDTH), BF16),
            pltpu.VMEM((2, NZ, ROWS, WIDTH), BF16),
            pltpu.VMEM((2 * NZ, ROWS, WIDTH), BF16),
            pltpu.VMEM((NZ, ROWS, WIDTH), BF16),
            pltpu.VMEM((NEP * SLOTS, WIDTH), BF16),
            pltpu.VMEM((TOKENS, WIDTH), F32),
            pltpu.VMEM((32, CHANNELS), BF16),
            pltpu.VMEM((32, CHANNELS), BF16),
            pltpu.VMEM((TOKENS + 32, CHANNELS), F32),
            pltpu.VMEM((TILE, CHANNELS), F32),
            pltpu.VMEM((TOKENS, CHANNELS), BF16),
            dma((11,)), dma((13,)),
            dma((2 * NZ,)), dma((2 * NZ,)), dma, dma((2, 2 * NZ)), dma, dma((2 * NZ,)),
            dma, dma((2, NZ)), dma, dma((2, NZ)), dma, dma((NZ,)), dma, dma,
        ],
        compiler_params=pltpu.CompilerParams(collective_id=0, has_side_effects=True, vmem_limit_bytes=46 * 1024 * 1024),
        name="filter_and_experts",
    )(*(pltpu.with_memory_space_constraint(argument, pltpu.HBM) for argument in arguments))
    return pl.pallas_call(
        hand_over,
        out_shape=shapes,
        in_specs=[vmem] * 2,
        out_specs=(hbm, hbm),
        scratch_shapes=[dma((2,))],
        compiler_params=pltpu.CompilerParams(vmem_limit_bytes=4 * 1024 * 1024),
        name="hand_over",
    )(*(pltpu.with_memory_space_constraint(result, pltpu.VMEM) for result in results))


def solution(mesh):
    in_specs = (
        P(("ep", "tp"), None),
        P(("ep", "tp"), None),
        P(),
        P(),
        P(),
        P(),
        P(),
        P(),
        P("ep", None),
        P(),
        P("ep", None),
        P("ep", None),
        P("ep", None, "tp"),
        P("ep", None, "tp"),
        P("ep", "tp", None),
    )
    out_specs = (P(("ep", "tp"), None), P("ep", "tp"))
    return jax.shard_map(local, mesh=mesh, in_specs=in_specs, out_specs=out_specs, check_vma=False)
```
